256 devices in a mesh: ep: 64 (over z, x, core), tp: 4 (over y).
Axes of the slice: x: 4, y: 4, z: 8, core: 2. Of those that a mesh axis runs over, the one named last changes fastest.
Arguments:
- queries: bfloat16 [16384, 1024], P('ep', 'tp'), may hold values from -256 to 256
- key_rows: bfloat16 [16384, 1024], P('ep', 'tp'), may hold values from -8 to 8
- value_rows: bfloat16 [16384, 1024], P('ep', 'tp'), may hold values from -6 to 6
- head_lambda: float32 [8], P('tp'), may hold values from 0.3 to 0.8
- sub_gain: float32 [128], replicated, may hold values from 0.1 to 1.9
- out_weight: bfloat16 [1024, 2048], P('tp'), may hold values from -0.1875 to 0.1875
- expert_input: bfloat16 [12288, 2048], P('ep'), may hold values from -6 to 6
- norm_gain: float32 [2048], replicated, may hold values from 0.1 to 1.9
- route_ids: int32 [12288, 2], P('ep'), may hold values from 0 to 63, all different within a row; in each aligned block of 192 rows (0 to 191, 192 to 383, ...) at most 10 rows name the same one
- route_weight: float32 [12288, 2], P('ep'), may hold values from 0.25 to 1
- gate_weight: bfloat16 [64, 2048, 3584], P('ep', None, 'tp'), may hold values from -0.125 to 0.125
- up_weight: bfloat16 [64, 2048, 3584], P('ep', None, 'tp'), may hold values from -0.125 to 0.125
- down_weight: bfloat16 [64, 3584, 2048], P('ep', 'tp'), may hold values from -0.09375 to 0.09375
Outputs:
- mixer_out: bfloat16 [16384, 2048], P(('ep', 'tp'))
- expert_out: bfloat16 [12288, 2048], P('ep', 'tp')
The draws below stay inside these ranges and needn't reach their ends.
Inputs may be any that keep to these rules, and one draw needn't show every extreme that they name: `route_ids`: each row names 2 different experts. In each aligned block of 192 rows no expert is named by more than 10 rows, a bound that some block reaches.
All inputs are finite; a program needn't handle non-finite values.
Results may differ from the reference program's by a relative error of at most 0.014.
Values may be sent and summed in bfloat16 or wider, within the bound.
A program may use at most 256 MiB of HBM per device.

```python
import math
import jax
import jax.numpy as jnp
import numpy as np
from jax import lax

D = 2048
HEADS = 8
HEAD_DIM = 64
VALUE_DIM = 128
FF = 3584
TOP = 2
TOK_B_DEV = 192
EXPERTS = 64
CAP = 10
TOKENS_A = 16384
TOKENS_B = 12288
N_EP = 64
N_TP = 4


def query_key_pair(key):
    base = jax.random.fold_in(key, 11)
    key_draw, query_draw = jax.random.split(base, 2)
    shape = (TOKENS_A, HEADS, 2, HEAD_DIM)
    key_vals = 1.3 * jax.random.truncated_normal(key_draw, -6.0, 6.0, shape, jnp.float32)
    query_vals = 1.3 * jax.random.truncated_normal(query_draw, -6.0, 6.0, shape, jnp.float32)
    return (query_vals.reshape(TOKENS_A, HEADS * 2 * HEAD_DIM), key_vals.reshape(TOKENS_A, HEADS * 2 * HEAD_DIM))


def draw_queries(key, part):
    return query_key_pair(key)[0].astype(jnp.bfloat16)


def draw_key_rows(key, part):
    return query_key_pair(key)[1].astype(jnp.bfloat16)


def block_scale(stream_key, dims, cuts, smallest, largest):
    loudness, own = 1.0, jax.random.fold_in(stream_key, 6)
    for position, parts in cuts:
        draws = jnp.exp(jax.random.uniform(jax.random.fold_in(own, position), (parts,), jnp.float32, smallest / len(cuts), largest / len(cuts)))
        loudness = loudness * jnp.repeat(draws, dims[position] // parts).reshape([-1 if axis == position else 1 for axis in range(len(dims))])
    return loudness


def shared_out(stream_key, own, number, rows, count, top, limit, skew):
    order = jax.random.permutation(stream_key, count)
    heavy_load, usual = portions_of(count, rows * top, limit, skew, True), portions_of(count, rows * top, limit, skew, False)
    places = jnp.arange(count)

    def named(lengths, offset_by):
        used = int((lengths > 0).sum())
        fixed = max(1, used // 4)
        passed = fixed + (places - fixed + offset_by * (used - fixed)) % max(1, count - fixed)
        return jnp.zeros((count,), jnp.int32).at[order[jnp.where(places < fixed, places, passed)]].set(jnp.asarray(lengths, jnp.int32))

    lengths = jnp.where(number % 4 == 0, named(heavy_load, number // 4), named(usual, number - number // 4 - 1))
    mixed = jax.random.permutation(jax.random.fold_in(own, 3), count)
    source_of, receiver = mixed[0:count // 2 * 2:2], mixed[1:count // 2 * 2:2]
    slack = jnp.minimum(lengths[source_of] - 1, limit - lengths[receiver]) // 2
    slack = jnp.where((source_of == order[0]) | (receiver == order[0]) | (lengths[receiver] == 0), 0, jnp.maximum(slack, 0))
    passed = jax.random.randint(jax.random.fold_in(own, 4), (count // 2,), 0, 1 << 20) % (slack + 1)
    lengths = lengths.at[source_of].add(-passed).at[receiver].add(passed)
    items = jnp.searchsorted(jnp.cumsum(lengths), jnp.arange(rows * top), side="right").astype(jnp.int32)
    grid = items.reshape(top, rows).T
    grid = grid[jax.random.permutation(jax.random.fold_in(own, 1), rows)]
    offset_by = jax.random.randint(jax.random.fold_in(own, 2), (rows, 1), 0, top)
    return jnp.take_along_axis(grid, (jnp.arange(top)[None, :] + offset_by) % top, axis=1)


def portions_of(amount, total, limit, skew, full):
    loads = [(1 << 20) // math.isqrt(standing ** skew) + 1 for standing in range(1, amount + 1)]
    largest = limit if full else min(limit, max(-(-total // amount), total * loads[0] // sum(loads)))
    least = 1 if total - largest >= amount - 1 else 0
    holding, rest = [largest] + [least] * (amount - 1), total - largest - least * (amount - 1)
    while rest > 0:
        free = [i for i in range(1, amount) if holding[i] < largest] or [i for i in range(1, amount) if holding[i] < limit]
        whole, budget = sum([loads[i] for i in free]), rest
        for i in free:
            addition = min(limit - holding[i], max(1, budget * loads[i] // whole), rest)
            holding[i] = holding[i] + addition
            rest = rest - addition
    return np.array(holding)


def noise(key, shape, spread, reach, shards=(), kind=jnp.bfloat16):
    level = block_scale(key, shape, shards, -0.22, 0.18) if shards else 1.0
    entries = jax.random.normal(key, shape, jnp.float32) * spread * level
    return jnp.minimum(jnp.maximum(entries, -reach), reach).astype(kind)


def setup_inputs(seed: int = 0) -> dict:
    arg_keys = jax.random.split(jax.random.key(seed), 14)
    queries = draw_queries(jax.random.fold_in(arg_keys[13], 71), 0)
    key_rows = draw_key_rows(jax.random.fold_in(arg_keys[13], 71), 0)
    value_rows = noise(arg_keys[2], (TOKENS_A, HEADS * VALUE_DIM), 1.0, 6.0, ((0, 64), (1, 4)))
    head_lambda = jnp.clip(0.3 + 0.5 * jax.random.uniform(arg_keys[3], (HEADS,), jnp.float32) ** block_scale(arg_keys[3], (HEADS,), ((0, 4),), -0.2, 0.2), 0.3, 0.8)
    sub_gain = jnp.clip(1.0 + 0.18 * jax.random.normal(arg_keys[4], (VALUE_DIM,), jnp.float32), 0.1, 1.9)
    out_weight = noise(arg_keys[5], (HEADS * VALUE_DIM, D), (HEADS * VALUE_DIM) ** -0.5, 0.1875, ((0, 4),))
    expert_input = noise(arg_keys[6], (TOKENS_B, D), 1.0, 6.0, ((0, 64),))
    norm_gain = jnp.clip(1.0 + 0.18 * jax.random.normal(arg_keys[7], (D,), jnp.float32), 0.1, 1.9)
    route_ids_keys = jax.random.split(jax.random.fold_in(arg_keys[8], 1), TOKENS_B // TOK_B_DEV)
    route_ids_turns = jax.random.permutation(jax.random.fold_in(arg_keys[8], 3), TOKENS_B // TOK_B_DEV)
    route_ids = jax.vmap(lambda own, number: shared_out(jax.random.fold_in(arg_keys[8], 2), own, number, TOK_B_DEV, EXPERTS, TOP, CAP, 1))(route_ids_keys, route_ids_turns).reshape((TOKENS_B, TOP))
    route_weight = jnp.clip(0.25 + 0.75 * jax.random.uniform(arg_keys[9], (TOKENS_B, TOP), jnp.float32) ** block_scale(arg_keys[9], (TOKENS_B, TOP), ((0, 64),), -0.2, 0.2), 0.25, 1.0)
    gate_weight = noise(arg_keys[10], (EXPERTS, D, FF), D ** -0.5, 0.125, ((0, 64), (2, 4)))
    up_weight = noise(arg_keys[11], (EXPERTS, D, FF), D ** -0.5, 0.125, ((0, 64), (2, 4)))
    down_weight = noise(arg_keys[12], (EXPERTS, FF, D), FF ** -0.5, 0.09375, ((0, 64), (1, 4)))
    return {"queries": queries, "key_rows": key_rows, "value_rows": value_rows, "head_lambda": head_lambda, "sub_gain": sub_gain, "out_weight": out_weight, "expert_input": expert_input, "norm_gain": norm_gain, "route_ids": route_ids, "route_weight": route_weight, "gate_weight": gate_weight, "up_weight": up_weight, "down_weight": down_weight}


EPS = 1e-06

def round_keep(values):
    return lax.optimization_barrier(values.astype(jnp.bfloat16)).astype(jnp.float32)

def head_output(query_head, key_head, value_head, lam_value, sub_gain):
    block_rows = math.gcd(TOKENS_A, 512)
    scaling = HEAD_DIM ** (-0.5)
    key_pos = jnp.arange(TOKENS_A, dtype=jnp.int32)
    key_wide = key_head.astype(jnp.float32)
    value_wide = value_head.astype(jnp.float32)

    def one_block(block_index):
        first_row = (block_index * block_rows).astype(jnp.int32)
        query_block = lax.dynamic_slice_in_dim(query_head, first_row, block_rows, 0).astype(jnp.float32)
        scores = jnp.einsum('qmd,kmd->mqk', query_block, key_wide) * scaling
        query_pos = first_row + jnp.arange(block_rows, dtype=jnp.int32)
        allowed = query_pos[:, None] >= key_pos[None, :]
        scores = jnp.where(allowed, scores, -jnp.inf)
        row_max = lax.optimization_barrier(jnp.max(scores, axis=-1, keepdims=True))
        weights = jnp.where(allowed, jnp.exp(scores - row_max), 0.0)
        row_total = lax.optimization_barrier(jnp.sum(weights, axis=-1))
        numerator = jnp.einsum('mqk,kd->mqd', round_keep(weights), value_wide)
        per_map = numerator / row_total[..., None]
        contrast = per_map[0] - lam_value * per_map[1]
        normed = contrast * lax.rsqrt(lax.optimization_barrier(jnp.mean(contrast * contrast, axis=-1, keepdims=True)) + EPS) * sub_gain
        return normed.astype(jnp.bfloat16)
    blocks = lax.map(one_block, jnp.arange(TOKENS_A // block_rows, dtype=jnp.int32))
    return blocks.reshape(TOKENS_A, VALUE_DIM)

def reference(queries, key_rows, value_rows, head_lambda, sub_gain, out_weight, expert_input, norm_gain, route_ids, route_weight, gate_weight, up_weight, down_weight):
    query_heads = jnp.moveaxis(queries.reshape(TOKENS_A, HEADS, 2, HEAD_DIM), 1, 0)
    key_heads = jnp.moveaxis(key_rows.reshape(TOKENS_A, HEADS, 2, HEAD_DIM), 1, 0)
    value_heads = jnp.moveaxis(value_rows.reshape(TOKENS_A, HEADS, VALUE_DIM), 1, 0)

    def per_head(operands):
        return head_output(operands[0], operands[1], operands[2], operands[3], sub_gain)
    attended = lax.map(per_head, (query_heads, key_heads, value_heads, head_lambda))
    attended = jnp.moveaxis(attended, 0, 1).reshape(TOKENS_A, HEADS * VALUE_DIM)
    group_cols = HEADS // N_TP * VALUE_DIM
    mixed_sum = jnp.zeros((TOKENS_A, D), jnp.float32)
    for group_index in range(N_TP):
        lower = group_index * group_cols
        share = jnp.dot(attended[:, lower:lower + group_cols], out_weight[lower:lower + group_cols], preferred_element_type=jnp.float32)
        mixed_sum = mixed_sum + round_keep(share)
    mixer_out = mixed_sum.astype(jnp.bfloat16)
    wide_rows = expert_input.astype(jnp.float32)
    normed_input = (wide_rows * lax.rsqrt(lax.optimization_barrier(jnp.mean(wide_rows * wide_rows, axis=-1, keepdims=True)) + EPS) * norm_gain).astype(jnp.bfloat16)
    flat_ids = route_ids.reshape(N_EP, TOK_B_DEV * TOP)
    onehot = (flat_ids[..., None] == jnp.arange(EXPERTS, dtype=jnp.int32)).astype(jnp.int32)
    rank_before = jnp.cumsum(onehot, axis=1) - onehot
    slot_index = lax.optimization_barrier(jnp.sum(rank_before * onehot, axis=-1))
    source = jnp.arange(N_EP, dtype=jnp.int32)[:, None]
    buffer_pos = ((flat_ids * N_EP + source) * CAP + slot_index).astype(jnp.int32)
    token_index = (source * TOK_B_DEV + jnp.arange(TOK_B_DEV * TOP, dtype=jnp.int32)[None, :] // TOP).astype(jnp.int32)
    row_table = jnp.full((EXPERTS * N_EP * CAP,), TOKENS_B, jnp.int32)
    row_table = row_table.at[buffer_pos.reshape(-1)].set(token_index.reshape(-1))
    padded = jnp.concatenate([normed_input, jnp.zeros((1, D), jnp.bfloat16)], axis=0)
    unit_share = FF // N_TP

    def one_expert(operands):
        gathered = padded[operands[0]]
        gate_act = jnp.dot(gathered, operands[1], preferred_element_type=jnp.float32)
        up_act = jnp.dot(gathered, operands[2], preferred_element_type=jnp.float32)
        hidden = (jax.nn.silu(gate_act) * up_act).astype(jnp.bfloat16)
        result_sum = jnp.zeros((N_EP * CAP, D), jnp.float32)
        for group_index in range(N_TP):
            lower = group_index * unit_share
            share = jnp.dot(hidden[:, lower:lower + unit_share], operands[3][lower:lower + unit_share], preferred_element_type=jnp.float32)
            result_sum = result_sum + round_keep(share)
        return result_sum.astype(jnp.bfloat16)
    results = lax.map(one_expert, (row_table.reshape(EXPERTS, N_EP * CAP), gate_weight, up_weight, down_weight))
    picked = results.reshape(EXPERTS * N_EP * CAP, D)[buffer_pos.reshape(-1)]
    picked = picked.reshape(TOKENS_B, TOP, D).astype(jnp.float32)
    expert_out = lax.optimization_barrier(jnp.sum(picked * route_weight[..., None], axis=1)).astype(jnp.bfloat16)
    return (mixer_out, expert_out)
```

```python
import functools
import math

import jax
import jax.numpy as jnp
from jax import lax
from jax.experimental import pallas as pl
from jax.experimental.pallas import tpu as pltpu
from jax.sharding import Mesh, PartitionSpec as P

EPS = 1e-06
NZ, NX, NC, NT = 8, 4, 2, 4
EP = ("z", "x", "core")
BLOCK = 256
HALF = BLOCK // 2
CHUNK = NC * BLOCK
COLS = 2 * NX * HALF
ACC = 144
LOW = -1e30
EXP2_SCALE = 64 ** (-0.5) * math.log2(math.e)


def pieces_of(value):
    first = value.astype(jnp.bfloat16).astype(jnp.float32)
    second = (value - first).astype(jnp.bfloat16).astype(jnp.float32)
    third = value - first - second
    return first, second, third


def flash_kernel(query_ref, pair_ref, out_ref, rhs_ref, max_ref, acc_ref):
    z, x, core = lax.axis_index("z"), lax.axis_index("x"), lax.axis_index("core")
    map_row = lax.broadcasted_iota(jnp.int32, (128, HALF), 0)
    ones = jnp.ones((ACC - 128, CHUNK), jnp.bfloat16)
    tile = 256

    for group in range(2):
        query_z = z if group == 0 else NZ - 1 - z
        for head in range(2):
            for step in range(NX):
                block = query_ref[group, step, head * 128 : (head + 1) * 128, :]
                for which in range(2):
                    first = (which * NX + step) * HALF
                    keep = (map_row < 64) if which == 0 else (map_row >= 64)
                    rhs_ref[:, first : first + HALF] = jnp.where(
                        keep, block, jnp.zeros_like(block)
                    )
            max_ref[...] = jnp.full_like(max_ref, LOW)
            acc_ref[...] = jnp.zeros_like(acc_ref)

            def work(step_z, masked):
                keys, values = [], []
                for c in range(NC):
                    keys.append(
                        pair_ref[step_z * NC + c, 0:256, head * 128 : (head + 1) * 128]
                    )
                    values.append(
                        pair_ref[step_z * NC + c, 256 + head * 128 : 256 + (head + 1) * 128, :]
                    )
                keys = jnp.concatenate(keys, axis=0)
                values = jnp.concatenate([jnp.concatenate(values, axis=1), ones], axis=0)
                for first in range(0, COLS, tile):
                    cols = slice(first, first + tile)
                    scores = jnp.dot(keys, rhs_ref[:, cols], preferred_element_type=jnp.float32)
                    if masked:
                        key = lax.broadcasted_iota(jnp.int32, (CHUNK, tile), 0)
                        key = key + 2 * BLOCK * x
                        col = lax.broadcasted_iota(jnp.int32, (CHUNK, tile), 1) + first
                        shift = (col // HALF) % NX
                        query_x = lax.rem(x - shift + NX, NX)
                        position = (2 * query_x + core) * BLOCK + group * HALF + col % HALF
                        scores = jnp.where(position >= key, scores, -3e38)
                    before = max_ref[0:1, cols]
                    now = jnp.maximum(before, jnp.max(scores, axis=0, keepdims=True))
                    weights = jnp.exp2((scores - now) * EXP2_SCALE).astype(jnp.bfloat16)
                    rescale = jnp.exp2((before - now) * EXP2_SCALE)
                    max_ref[0:1, cols] = now
                    acc_ref[:, cols] = acc_ref[:, cols] * rescale + jnp.dot(
                        values, weights, preferred_element_type=jnp.float32
                    )

            lax.fori_loop(0, query_z, lambda s, c: (work(s, False), c)[1], 0)
            work(query_z, True)

            row = lax.broadcasted_iota(jnp.int32, (ACC - 128, COLS), 0)
            stats = jnp.zeros((ACC - 128, COLS), jnp.float32)
            rows = pieces_of(acc_ref[128:129, :]) + pieces_of(max_ref[0:1, :])
            for index, piece in enumerate(rows):
                stats = jnp.where(row == index, piece, stats)
            for which in range(2):
                for step in range(NX):
                    first = (which * NX + step) * HALF
                    lanes = slice(group * HALF, (group + 1) * HALF)
                    out_ref[step, 2 * head + which, 0:128, lanes] = acc_ref[
                        0:128, first : first + HALF
                    ].astype(jnp.bfloat16)
                    out_ref[step, 2 * head + which, 128:ACC, lanes] = stats[
                        :, first : first + HALF
                    ].astype(jnp.bfloat16)


def flash(query_parts, pairs):
    return pl.pallas_call(
        flash_kernel,
        out_shape=jax.ShapeDtypeStruct((NX, 4, ACC, BLOCK), jnp.bfloat16),
        in_specs=[pl.BlockSpec(memory_space=pltpu.VMEM)] * 2,
        out_specs=pl.BlockSpec(memory_space=pltpu.VMEM),
        scratch_shapes=[
            pltpu.VMEM((128, COLS), jnp.bfloat16),
            pltpu.VMEM((8, COLS), jnp.float32),
            pltpu.VMEM((ACC, COLS), jnp.float32),
        ],
        compiler_params=pltpu.CompilerParams(vmem_limit_bytes=40 * 2**20),
        cost_estimate=pl.CostEstimate(
            flops=15_000_000_000, bytes_accessed=6_000_000, transcendentals=9_400_000
        ),
        name="flash",
    )(query_parts, pairs)


def merge_kernel(lambda_ref, gain_ref, own_ref, one_ref, two_ref, three_ref, out_ref):
    parts = (own_ref, one_ref, two_ref, three_ref)
    for head in range(2):
        per_map = []
        for which in range(2):
            index = 2 * head + which
            totals, maxima = [], []
            for part in parts:
                stats = part[index, 128:ACC, :].astype(jnp.float32)
                totals.append(stats[0:1] + stats[1:2] + stats[2:3])
                maxima.append(stats[3:4] + stats[4:5] + stats[5:6])
            largest = functools.reduce(jnp.maximum, maxima)
            total, numerator = 0.0, 0.0
            for part, own_total, own_max in zip(parts, totals, maxima):
                factor = jnp.exp2((own_max - largest) * EXP2_SCALE)
                total = total + factor * own_total
                numerator = numerator + factor * part[index, 0:128, :].astype(jnp.float32)
            per_map.append(numerator / total)
        contrast = per_map[0] - lambda_ref[head] * per_map[1]
        square = jnp.mean(contrast * contrast, axis=0, keepdims=True)
        normed = contrast * lax.rsqrt(square + EPS) * gain_ref[...]
        out_ref[head * 128 : (head + 1) * 128, :] = normed.astype(jnp.bfloat16)


def merge(head_lambda, sub_gain, parts):
    return pl.pallas_call(
        merge_kernel,
        out_shape=jax.ShapeDtypeStruct((BLOCK, BLOCK), jnp.bfloat16),
        in_specs=[pl.BlockSpec(memory_space=pltpu.SMEM)]
        + [pl.BlockSpec(memory_space=pltpu.VMEM)] * 5,
        out_specs=pl.BlockSpec(memory_space=pltpu.VMEM),
        name="merge",
    )(head_lambda, sub_gain[:, None], *parts)


def moved(array, shift, flip):
    pairs = []
    for z in range(NZ):
        for x in range(NX):
            to_z = NZ - 1 - z if flip else z
            pairs.append((z * NX + x, to_z * NX + (x + shift) % NX))
    return lax.ppermute(array, ("z", "x"), pairs)


def mixer_half(queries, key_rows, value_rows, head_lambda, sub_gain, out_weight):
    pair = jnp.concatenate([key_rows, value_rows.T], axis=0)
    pairs = lax.all_gather(pair, ("z", "core"), axis=0, tiled=False)
    flipped = queries.T
    lower, upper = flipped[:, :HALF], flipped[:, HALF:]
    parts = [lower] + [moved(lower, s, False) for s in range(1, NX)]
    parts += [moved(upper, s, True) for s in range(NX)]
    query_parts = jnp.stack(parts).reshape(2, NX, BLOCK, HALF)
    partial = flash(query_parts, pairs)
    parts = [partial[0]] + [moved(partial[s], -s, False) for s in range(1, NX)]
    attended = merge(head_lambda, sub_gain, parts)
    attended = jnp.concatenate(
        [attended[:, :HALF], moved(attended[:, HALF:], 0, True)], axis=1
    )
    part = lax.dot_general(
        attended, out_weight, (((0,), (0,)), ((), ())), preferred_element_type=jnp.float32
    ).astype(jnp.bfloat16)
    return lax.psum_scatter(part, "tp", scatter_dimension=0, tiled=True)


def expert_half(
    expert_input, norm_gain, route_ids, route_weight, gate_weight, up_weight, down_weight
):
    rows_here, model_width = expert_input.shape
    experts = lax.axis_size(EP)
    top_count = route_ids.shape[1]
    capacity = 5 * top_count * rows_here // (3 * experts)
    slots = experts * capacity
    wide_rows = expert_input.astype(jnp.float32)
    normed = (
        wide_rows
        * lax.rsqrt(jnp.mean(wide_rows * wide_rows, axis=-1, keepdims=True) + EPS)
        * norm_gain
    ).astype(jnp.bfloat16)
    flat_ids = route_ids.reshape(-1)
    onehot = (flat_ids[:, None] == jnp.arange(experts, dtype=jnp.int32)[None, :]).astype(jnp.int32)
    rank_before = jnp.cumsum(onehot, axis=0) - onehot
    slot_index = jnp.sum(rank_before * onehot, axis=1)
    buffer_pos = (flat_ids * capacity + slot_index).reshape(rows_here, top_count)
    matches = buffer_pos[None, :, :] == jnp.arange(slots, dtype=jnp.int32)[:, None, None]
    dispatch = jnp.any(matches, axis=-1).astype(jnp.bfloat16)
    combine = jnp.sum(jnp.where(matches, route_weight[None, :, :], 0.0), axis=-1)
    gate_mat = gate_weight[0]
    up_mat = up_weight[0]
    down_mat = down_weight[0]
    column_share = model_width // lax.axis_size("tp")
    own_cols = lax.dynamic_slice_in_dim(
        normed, lax.axis_index("tp") * column_share, column_share, 1
    )
    outgoing = jnp.dot(dispatch, own_cols, preferred_element_type=jnp.float32).astype(jnp.bfloat16)
    arrived = lax.all_to_all(
        outgoing.reshape(experts, capacity, column_share),
        EP,
        split_axis=0,
        concat_axis=0,
        tiled=True,
    ).reshape(slots, column_share)
    pieces = lax.all_gather(arrived, "tp", axis=0, tiled=False)
    pieces = jnp.moveaxis(pieces, 0, 1).reshape(slots, model_width)
    gate_act = jnp.dot(pieces, gate_mat, preferred_element_type=jnp.float32)
    up_act = jnp.dot(pieces, up_mat, preferred_element_type=jnp.float32)
    hidden = (jax.nn.silu(gate_act) * up_act).astype(jnp.bfloat16)
    partial_result = jnp.dot(hidden, down_mat, preferred_element_type=jnp.float32)
    summed = lax.psum_scatter(
        partial_result.astype(jnp.bfloat16), "tp", scatter_dimension=1, tiled=True
    )
    col_count = summed.shape[1]
    returned = lax.all_to_all(
        summed.reshape(experts, capacity, col_count), EP, split_axis=0, concat_axis=0, tiled=True
    ).reshape(slots, col_count)
    mixed = lax.dot_general(
        combine,
        returned.astype(jnp.float32),
        (((0,), (0,)), ((), ())),
        preferred_element_type=jnp.float32,
    )
    return mixed.astype(jnp.bfloat16)


def shards(
    queries,
    key_rows,
    value_rows,
    head_lambda,
    sub_gain,
    out_weight,
    expert_input,
    norm_gain,
    route_ids,
    route_weight,
    gate_weight,
    up_weight,
    down_weight,
):
    mixer_out = mixer_half(queries, key_rows, value_rows, head_lambda, sub_gain, out_weight)
    expert_out = expert_half(
        expert_input, norm_gain, route_ids, route_weight, gate_weight, up_weight, down_weight
    )
    return (mixer_out, expert_out)


def solution(mesh):
    mesh = Mesh(mesh.devices.reshape(NZ, NX, NC, NT), (*EP, "tp"))
    placed = (
        P(EP, "tp"),
        P(EP, "tp"),
        P(EP, "tp"),
        P("tp"),
        P(),
        P("tp", None),
        P(EP, None),
        P(),
        P(EP, None),
        P(EP, None),
        P(EP, None, "tp"),
        P(EP, None, "tp"),
        P(EP, "tp", None),
    )
    return jax.shard_map(
        shards,
        mesh=mesh,
        in_specs=placed,
        out_specs=(P((*EP, "tp"), None), P(EP, "tp")),
        check_vma=False,
    )
```

```python
import functools
import math

import jax
import jax.numpy as jnp
from jax import lax
from jax.experimental import pallas as pl
from jax.experimental.pallas import tpu as pltpu
from jax.sharding import Mesh, PartitionSpec as P

EPS = 1e-06
NZ, NX, NC, NT = 8, 4, 2, 4
EP = ("z", "x", "core")
BLOCK = 256
HALF = BLOCK // 2
CHUNK = NC * BLOCK
COLS = 2 * NX * HALF
ACC = 144
COLS_T = 512
FULL, TAIL = 8, 2
NEAR = (0, 1, 7, 2, 6, 3, 5, 4)
PLUS = (0, 7, 6, 5)
LOW = -1e30
EXP2_SCALE = 64 ** (-0.5) * math.log2(math.e)


def pieces_of(value):
    first = value.astype(jnp.bfloat16).astype(jnp.float32)
    second = (value - first).astype(jnp.bfloat16).astype(jnp.float32)
    third = value - first - second
    return first, second, third


def flash_kernel(query_ref, pair_ref, out_ref, rhs_ref, max_ref, acc_ref):
    z, x, core = lax.axis_index("z"), lax.axis_index("x"), lax.axis_index("core")
    map_row = lax.broadcasted_iota(jnp.int32, (128, HALF), 0)
    ones = jnp.ones((ACC - 128, CHUNK), jnp.bfloat16)
    tile = 256

    for group in range(2):
        query_z = z if group == 0 else NZ - 1 - z
        for head in range(2):
            for step in range(NX):
                block = query_ref[group, step, head * 128 : (head + 1) * 128, :]
                for which in range(2):
                    first = (which * NX + step) * HALF
                    keep = (map_row < 64) if which == 0 else (map_row >= 64)
                    rhs_ref[:, first : first + HALF] = jnp.where(
                        keep, block, jnp.zeros_like(block)
                    )
            max_ref[...] = jnp.full_like(max_ref, LOW)
            acc_ref[...] = jnp.zeros_like(acc_ref)

            def work(step_z, masked):
                keys, values = [], []
                for c in range(NC):
                    keys.append(
                        pair_ref[step_z * NC + c, 0:256, head * 128 : (head + 1) * 128]
                    )
                    values.append(
                        pair_ref[step_z * NC + c, 256 + head * 128 : 256 + (head + 1) * 128, :]
                    )
                keys = jnp.concatenate(keys, axis=0)
                values = jnp.concatenate([jnp.concatenate(values, axis=1), ones], axis=0)
                for first in range(0, COLS, tile):
                    cols = slice(first, first + tile)
                    scores = jnp.dot(keys, rhs_ref[:, cols], preferred_element_type=jnp.float32)
                    if masked:
                        key = lax.broadcasted_iota(jnp.int32, (CHUNK, tile), 0)
                        key = key + 2 * BLOCK * x
                        col = lax.broadcasted_iota(jnp.int32, (CHUNK, tile), 1) + first
                        shift = (col // HALF) % NX
                        query_x = lax.rem(x - shift + NX, NX)
                        position = (2 * query_x + core) * BLOCK + group * HALF + col % HALF
                        scores = jnp.where(position >= key, scores, -3e38)
                    before = max_ref[0:1, cols]
                    now = jnp.maximum(before, jnp.max(scores, axis=0, keepdims=True))
                    weights = jnp.exp2((scores - now) * EXP2_SCALE).astype(jnp.bfloat16)
                    rescale = jnp.exp2((before - now) * EXP2_SCALE)
                    max_ref[0:1, cols] = now
                    acc_ref[:, cols] = acc_ref[:, cols] * rescale + jnp.dot(
                        values, weights, preferred_element_type=jnp.float32
                    )

            lax.fori_loop(0, query_z, lambda s, c: (work(s, False), c)[1], 0)
            work(query_z, True)

            row = lax.broadcasted_iota(jnp.int32, (ACC - 128, COLS), 0)
            stats = jnp.zeros((ACC - 128, COLS), jnp.float32)
            rows = pieces_of(acc_ref[128:129, :]) + pieces_of(max_ref[0:1, :])
            for index, piece in enumerate(rows):
                stats = jnp.where(row == index, piece, stats)
            for which in range(2):
                for step in range(NX):
                    first = (which * NX + step) * HALF
                    lanes = slice(group * HALF, (group + 1) * HALF)
                    out_ref[step, 2 * head + which, 0:128, lanes] = acc_ref[
                        0:128, first : first + HALF
                    ].astype(jnp.bfloat16)
                    out_ref[step, 2 * head + which, 128:ACC, lanes] = stats[
                        :, first : first + HALF
                    ].astype(jnp.bfloat16)


def flash(query_parts, pairs):
    return pl.pallas_call(
        flash_kernel,
        out_shape=jax.ShapeDtypeStruct((NX, 4, ACC, BLOCK), jnp.bfloat16),
        in_specs=[pl.BlockSpec(memory_space=pltpu.VMEM)] * 2,
        out_specs=pl.BlockSpec(memory_space=pltpu.VMEM),
        scratch_shapes=[
            pltpu.VMEM((128, COLS), jnp.bfloat16),
            pltpu.VMEM((8, COLS), jnp.float32),
            pltpu.VMEM((ACC, COLS), jnp.float32),
        ],
        compiler_params=pltpu.CompilerParams(vmem_limit_bytes=40 * 2**20),
        cost_estimate=pl.CostEstimate(
            flops=15_000_000_000, bytes_accessed=6_000_000, transcendentals=9_400_000
        ),
        name="flash",
    )(query_parts, pairs)


def places():
    return tuple(lax.axis_index(name) for name in (*EP, "tp"))


def remote(source, target, send, receive, device):
    return pltpu.make_async_remote_copy(
        src_ref=source,
        dst_ref=target,
        send_sem=send,
        recv_sem=receive,
        device_id=device,
        device_id_type=pl.DeviceIdType.MESH,
    )


def greet_all(z, x, c, t):
    me = (z * NX + x) * NC + c
    barrier = pltpu.get_barrier_semaphore()

    def signal(step, carry):
        peer = lax.rem(me + step, NZ * NX * NC)
        device = (peer // (NX * NC), lax.rem(peer // NC, NX), lax.rem(peer, NC), t)
        pl.semaphore_signal(
            barrier, inc=1, device_id=device, device_id_type=pl.DeviceIdType.MESH
        )
        return carry

    for dy in (1, NT - 1):
        pl.semaphore_signal(
            barrier,
            inc=1,
            device_id=(z, x, c, lax.rem(t + dy, NT)),
            device_id_type=pl.DeviceIdType.MESH,
        )
    lax.fori_loop(1, NZ * NX * NC, signal, 0)
    pl.semaphore_wait(barrier, NZ * NX * NC + 1)


def columns_of(t):
    return pl.ds(pl.multiple_of(t * COLS_T, COLS_T), COLS_T)


def dispatch_kernel(
    main_ref, tail_ref, pair_ref, query_ref, xmain, xtail, pairs, parts,
    own_sem, out_send, out_recv, y_send, y_recv, kv_send, kv_recv, c_send, c_recv, q_send, q_recv,
):
    z, x, c, t = places()
    me = (z * NX + x) * NC + c
    local = x * NC + c
    group = NX * NC
    after, before = lax.rem(t + 1, NT), lax.rem(t + NT - 1, NT)
    own = columns_of(t)
    own_copies = [
        pltpu.make_async_copy(main_ref.at[me], xmain.at[me, :, own], own_sem.at[0]),
        pltpu.make_async_copy(tail_ref.at[me], xtail.at[me, :, own], own_sem.at[1]),
        pltpu.make_async_copy(pair_ref, pairs.at[z * NC + c], own_sem.at[2]),
        pltpu.make_async_copy(query_ref.at[0], parts.at[0, 0], own_sem.at[3]),
    ]
    for copy in own_copies:
        copy.start()
    greet_all(z, x, c, t)

    for dz in (1, 7, 2, 6, 3, 5, 4, 0):
        to_z = lax.rem(z + dz, NZ)

        def send(step, carry):
            peer = lax.rem(local + step, group)
            device = (to_z, peer // NC, lax.rem(peer, NC), t)
            slab = to_z * group + peer
            for k, (source, target) in enumerate(((main_ref, xmain), (tail_ref, xtail))):
                remote(
                    source.at[slab], target.at[me, :, own],
                    out_send.at[k], out_recv.at[k, dz], device,
                ).start()
            return carry

        lax.fori_loop(1 if dz == 0 else 0, group, send, 0)

    mirrored = (NZ - 1 - z, x, c, t)
    remote(query_ref.at[1], parts.at[1, 0], q_send.at[3], q_recv.at[3], mirrored).start()
    for k in range(1, NX):
        device = (z, lax.rem(x + k, NX), c, t)
        remote(query_ref.at[0], parts.at[0, k], q_send.at[k - 1], q_recv.at[k - 1], device).start()

    up, down = (lax.rem(z + 1, NZ), x, c, t), (lax.rem(z + NZ - 1, NZ), x, c, t)
    across = (z, x, 1 - c, t)
    for way, device in enumerate((up, down)):
        remote(
            pair_ref, pairs.at[z * NC + c], kv_send.at[way, 0], kv_recv.at[way, 0], device
        ).start()
    remote(pair_ref, pairs.at[z * NC + c], c_send.at[0], c_recv.at[0], across).start()

    def rows_of(dz):
        return pl.ds(lax.rem(z - dz + NZ, NZ) * group, group)

    def y_copies(dz, slot, columns, device):
        rows = rows_of(dz)
        return [
            remote(
                target.at[rows, :, columns], target.at[rows, :, columns],
                y_send.at[slot, dz, k], y_recv.at[slot, dz, k], device,
            )
            for k, target in enumerate((xmain, xtail))
        ]

    to_after, to_before = (z, x, c, after), (z, x, c, before)

    def y_relay(dz):
        first = y_copies(dz, 0 if dz in PLUS else 1, own, to_after)
        for copy in first:
            copy.wait_recv()
        if dz in PLUS:
            copies = y_copies(dz, 2, columns_of(before), to_after)
        else:
            copies = y_copies(dz, 2, columns_of(after), to_before)
        for copy in copies:
            copy.start()

    def kv_step(step):
        for way, device in enumerate((up, down)):
            back = NZ - step if way == 0 else step
            block = lax.rem(z + back, NZ) * NC + c
            if step < 4:
                here = pairs.at[block]
                onward = here
                if step == 3:
                    onward = pairs.at[block, pl.ds(way * BLOCK, BLOCK), :]
            else:
                here = pairs.at[block, pl.ds(way * BLOCK, BLOCK), :]
            remote(
                here, here, kv_send.at[way, step - 1], kv_recv.at[way, step - 1], device
            ).wait_recv()
            if step < 4:
                remote(
                    onward, onward, kv_send.at[way, step], kv_recv.at[way, step], device
                ).start()
            slot = 2 * step - 1 + way
            remote(here, here, c_send.at[slot], c_recv.at[slot], across).start()

    for copy in own_copies:
        copy.wait()
    for index, dz in enumerate(NEAR):
        count = group - 1 if dz == 0 else group
        first = 0 if dz == 0 else lax.rem(z - dz + NZ, NZ) * group
        rows = pl.ds(first, count)
        for k, (source, target) in enumerate(((main_ref, xmain), (tail_ref, xtail))):
            remote(
                source.at[pl.ds(0, count)], target.at[rows, :, own],
                out_send.at[k], out_recv.at[k, dz], up,
            ).wait_recv()
        for slot, device in enumerate((to_after, to_before)):
            for copy in y_copies(dz, slot, own, device):
                copy.start()
        if index == 1:
            remote(
                query_ref.at[1], parts.at[1, 0], q_send.at[3], q_recv.at[3], mirrored
            ).wait_recv()
            for k in range(1, NX):
                device = (z, lax.rem(x + k, NX), c, t)
                remote(
                    parts.at[1, 0], parts.at[1, k], q_send.at[3 + k], q_recv.at[3 + k], device
                ).start()
        if index >= 2:
            y_relay(NEAR[index - 2])
    kv_step(1)
    y_relay(NEAR[6])
    y_relay(NEAR[7])
    for step in (2, 3, 4):
        kv_step(step)

    for dz in NEAR:
        for copy in y_copies(dz, 1 if dz in PLUS else 0, own, to_after):
            copy.wait_recv()
        for copy in y_copies(dz, 2, own, to_after):
            copy.wait_recv()
        for slot in range(3):
            for copy in y_copies(dz, slot, own, to_after):
                copy.wait_send()
    for k, (source, target) in enumerate(((main_ref, xmain), (tail_ref, xtail))):
        every = pl.ds(0, NZ * group - 1)
        remote(
            source.at[every], target.at[every, :, own], out_send.at[k], out_recv.at[k, 0], up
        ).wait_send()
    for way in range(2):
        for step in range(4):
            block = pairs.at[0] if step < 3 else pairs.at[0, pl.ds(0, BLOCK), :]
            remote(block, block, kv_send.at[way, step], kv_recv.at[way, step], up).wait_send()
    for slot in range(9):
        block = pairs.at[0] if slot < 7 else pairs.at[0, pl.ds(0, BLOCK), :]
        copy = remote(block, block, c_send.at[slot], c_recv.at[slot], across)
        copy.wait_send()
        copy.wait_recv()
    for slot in range(7):
        copy = remote(parts.at[0, 0], parts.at[0, 0], q_send.at[slot], q_recv.at[slot], up)
        copy.wait_send()
        if slot != 3:
            copy.wait_recv()


VMEM = pl.BlockSpec(memory_space=pltpu.VMEM)


def dispatch_call(main, tail, pair, queries):
    dma = pltpu.SemaphoreType.DMA
    slabs = NZ * NX * NC
    return pl.pallas_call(
        dispatch_kernel,
        out_shape=(
            jax.ShapeDtypeStruct((slabs, FULL, NT * COLS_T), jnp.bfloat16),
            jax.ShapeDtypeStruct((slabs, TAIL, NT * COLS_T), jnp.bfloat16),
            jax.ShapeDtypeStruct((NZ * NC, 2 * BLOCK, BLOCK), jnp.bfloat16),
            jax.ShapeDtypeStruct((2, NX, BLOCK, HALF), jnp.bfloat16),
        ),
        in_specs=[VMEM] * 4,
        out_specs=(VMEM,) * 4,
        scratch_shapes=[
            dma((4,)), dma((2,)), dma((2, NZ)), dma((3, NZ, 2)), dma((3, NZ, 2)),
            dma((2, 4)), dma((2, 4)), dma((9,)), dma((9,)), dma((7,)), dma((7,)),
        ],
        compiler_params=pltpu.CompilerParams(
            collective_id=0, has_side_effects=True, vmem_limit_bytes=24 * 2**20
        ),
        name="dispatch",
    )(main, tail, pair, queries)


def return_kernel(
    fmain, ftail, partial, rmain, rtail, parts,
    relay_main, relay_tail, sum_main, sum_tail, in_main, in_tail, red_main, red_tail,
    own_sem, p_send, p_recv, relay_send, relay_recv, y_send, y_recv, out_send, out_recv,
):
    z, x, c, t = places()
    me = (z * NX + x) * NC + c
    local = x * NC + c
    group = NX * NC
    after, before = lax.rem(t + 1, NT), lax.rem(t + NT - 1, NT)
    opposite = lax.rem(t + 2, NT)
    to_after, to_before = (z, x, c, after), (z, x, c, before)
    greet_all(z, x, c, t)
    far = NEAR[::-1]
    pairs = (
        (fmain, relay_main, sum_main, in_main, red_main, rmain),
        (ftail, relay_tail, sum_tail, in_tail, red_tail, rtail),
    )

    def rows_of(dz):
        return pl.ds(lax.rem(z + dz, NZ) * group, group)

    def relay_copy(dz, k):
        source, target = pairs[k][0], pairs[k][1]
        return remote(
            source.at[rows_of(dz), :, columns_of(opposite)], target.at[dz],
            relay_send.at[dz, k], relay_recv.at[dz, k],
            to_after if dz in PLUS else to_before,
        )

    def y_copy(dz, k, way, source):
        return remote(
            source, pairs[k][3].at[way, dz], y_send.at[way, dz, k], y_recv.at[way, dz, k],
            (to_after, to_before)[way],
        )

    def direct(dz, k):
        way = 1 if dz in PLUS else 0
        columns = columns_of((after, before)[way])
        return y_copy(dz, k, way, pairs[k][0].at[rows_of(dz), :, columns])

    for dz in far:
        for k in range(2):
            relay_copy(dz, k).start()
    for k in range(1, NX):
        device = (z, lax.rem(x + NX - k, NX), c, t)
        remote(partial.at[k], parts.at[k - 1], p_send.at[k - 1], p_recv.at[k - 1], device).start()
    for dz in far:
        for k in range(2):
            direct(dz, k).start()

    def add_relay(dz):
        way = 0 if dz in PLUS else 1
        columns = columns_of((after, before)[way])
        for k in range(2):
            relay_copy(dz, k).wait_recv()
            source, relayed, total = pairs[k][:3]
            mine = source[rows_of(dz), :, columns].astype(jnp.float32)
            total[dz] = (mine + relayed[dz].astype(jnp.float32)).astype(jnp.bfloat16)
            y_copy(dz, k, way, total.at[dz]).start()

    def finish(dz):
        to_z = lax.rem(z + dz, NZ)
        for k in range(2):
            source, arrived, reduced = pairs[k][0], pairs[k][3], pairs[k][4]
            for way in range(2):
                y_copy(dz, k, way, pairs[k][2].at[dz]).wait_recv()
            reduced[rows_of(dz)] = (
                source[rows_of(dz), :, columns_of(t)].astype(jnp.float32)
                + arrived[0, dz].astype(jnp.float32)
                + arrived[1, dz].astype(jnp.float32)
            ).astype(jnp.bfloat16)

        def send(step, carry):
            peer = lax.rem(local + step, group)
            device = (to_z, peer // NC, lax.rem(peer, NC), t)
            for k in range(2):
                remote(
                    pairs[k][4].at[to_z * group + peer], pairs[k][5].at[me],
                    out_send.at[k], out_recv.at[k], device,
                ).start()
            return carry

        lax.fori_loop(1 if dz == 0 else 0, group, send, 0)
        if dz == 0:
            for k in range(2):
                pltpu.make_async_copy(
                    pairs[k][4].at[me], pairs[k][5].at[me], own_sem.at[k]
                ).start()

    for index, dz in enumerate(far):
        add_relay(dz)
        if index >= 1:
            finish(far[index - 1])
    finish(far[-1])

    for k in range(2):
        pltpu.make_async_copy(pairs[k][4].at[me], pairs[k][5].at[me], own_sem.at[k]).wait()
        every = pl.ds(0, NZ * group - 1)
        copy = remote(
            pairs[k][4].at[every], pairs[k][5].at[every], out_send.at[k], out_recv.at[k], to_after
        )
        copy.wait_recv()
        copy.wait_send()
        for dz in far:
            relay_copy(dz, k).wait_send()
            for way in range(2):
                y_copy(dz, k, way, pairs[k][2].at[dz]).wait_send()
    for k in range(1, NX):
        copy = remote(partial.at[k], parts.at[k - 1], p_send.at[k - 1], p_recv.at[k - 1], to_after)
        copy.wait_recv()
        copy.wait_send()


def return_call(fmain, ftail, partial):
    dma = pltpu.SemaphoreType.DMA
    slabs = NZ * NX * NC
    group = NX * NC

    def both(*lead):
        return [
            pltpu.VMEM((*lead, rows, COLS_T), jnp.bfloat16) for rows in (FULL, TAIL)
        ]

    return pl.pallas_call(
        return_kernel,
        out_shape=(
            jax.ShapeDtypeStruct((slabs, FULL, COLS_T), jnp.bfloat16),
            jax.ShapeDtypeStruct((slabs, TAIL, COLS_T), jnp.bfloat16),
            jax.ShapeDtypeStruct((NX - 1, 4, ACC, BLOCK), jnp.bfloat16),
        ),
        in_specs=[VMEM] * 3,
        out_specs=(VMEM,) * 3,
        scratch_shapes=[
            *both(NZ, group), *both(NZ, group), *both(2, NZ, group), *both(slabs),
            dma((2,)), dma((3,)), dma((3,)), dma((NZ, 2)), dma((NZ, 2)),
            dma((2, NZ, 2)), dma((2, NZ, 2)), dma((2,)), dma((2,)),
        ],
        compiler_params=pltpu.CompilerParams(
            collective_id=1, has_side_effects=True, vmem_limit_bytes=24 * 2**20
        ),
        name="give_back",
    )(fmain, ftail, partial)


def hidden_kernel(xmain, xtail, gate, up, down, fmain, ftail, rows, hidden):
    count = xmain.shape[0]
    rows[0:count] = xmain[...]
    rows[count:] = xtail[...]
    width = gate.shape[1]
    for first in range(0, width, 256):
        cols = slice(first, min(first + 256, width))
        gate_act = jnp.dot(rows[...], gate[:, cols], preferred_element_type=jnp.float32)
        up_act = jnp.dot(rows[...], up[:, cols], preferred_element_type=jnp.float32)
        value = gate_act / (1.0 + jnp.exp(-gate_act)) * up_act
        hidden[:, cols] = value.astype(jnp.bfloat16)
    for first in range(0, fmain.shape[1], 256):
        cols = slice(first, first + 256)
        out = jnp.dot(hidden[...], down[:, cols], preferred_element_type=jnp.float32)
        fmain[:, cols] = out[0:count].astype(jnp.bfloat16)
        ftail[:, cols] = out[count:].astype(jnp.bfloat16)


def hidden_call(xmain, xtail, gate, up, down):
    return pl.pallas_call(
        hidden_kernel,
        out_shape=(
            jax.ShapeDtypeStruct(xmain.shape, jnp.bfloat16),
            jax.ShapeDtypeStruct(xtail.shape, jnp.bfloat16),
        ),
        in_specs=[VMEM] * 5,
        out_specs=(VMEM,) * 2,
        scratch_shapes=[
            pltpu.VMEM((xmain.shape[0] + xtail.shape[0], xmain.shape[1]), jnp.bfloat16),
            pltpu.VMEM((xmain.shape[0] + xtail.shape[0], gate.shape[1]), jnp.bfloat16),
        ],
        compiler_params=pltpu.CompilerParams(vmem_limit_bytes=32 * 2**20),
        cost_estimate=pl.CostEstimate(
            flops=7_000_000_000, bytes_accessed=16_000_000, transcendentals=600_000
        ),
        name="hidden",
    )(xmain, xtail, gate, up, down)


def mixer_kernel(
    lambda_ref, gain_ref, partial_ref, parts_ref, weight_ref, out_ref,
    attended, upper_send, upper_recv, blocks, relayed, totals, arrived,
    u_send, u_recv, relay_send, relay_recv, y_send, y_recv,
):
    z, x, c, t = places()
    after, before = lax.rem(t + 1, NT), lax.rem(t + NT - 1, NT)
    opposite = lax.rem(t + 2, NT)
    devices = ((z, x, c, after), (z, x, c, before))
    mirrored = (NZ - 1 - z, x, c, t)
    barrier = pltpu.get_barrier_semaphore()
    for device in (*devices, mirrored):
        pl.semaphore_signal(
            barrier, inc=1, device_id=device, device_id_type=pl.DeviceIdType.MESH
        )

    for head in range(2):
        per_map = []
        for which in range(2):
            index = 2 * head + which
            sources = [partial_ref.at[0, index]] + [parts_ref.at[k, index] for k in range(NX - 1)]
            totals_of, maxima = [], []
            for part in sources:
                stats = part[128:ACC, :].astype(jnp.float32)
                totals_of.append(stats[0:1] + stats[1:2] + stats[2:3])
                maxima.append(stats[3:4] + stats[4:5] + stats[5:6])
            largest = functools.reduce(jnp.maximum, maxima)
            total, numerator = 0.0, 0.0
            for part, own_total, own_max in zip(sources, totals_of, maxima):
                factor = jnp.exp2((own_max - largest) * EXP2_SCALE)
                total = total + factor * own_total
                numerator = numerator + factor * part[0:128, :].astype(jnp.float32)
            per_map.append(numerator / total)
        contrast = per_map[0] - lambda_ref[head] * per_map[1]
        square = jnp.mean(contrast * contrast, axis=0, keepdims=True)
        normed = contrast * lax.rsqrt(square + EPS) * gain_ref[...]
        normed = normed.astype(jnp.bfloat16)
        attended[head * 128 : (head + 1) * 128, :] = normed[:, :HALF]
        upper_send[head * 128 : (head + 1) * 128, :] = normed[:, HALF:]

    pl.semaphore_wait(barrier, 3)
    flip = remote(upper_send, upper_recv, u_send, u_recv, mirrored)
    flip.start()
    rows = BLOCK // NT
    half = rows // 2

    def project(source, first):
        for low in range(0, 2048, 512):
            part = lax.dot_general(
                source[...], weight_ref[:, low : low + 512],
                (((0,), (0,)), ((), ())), preferred_element_type=jnp.float32,
            ).astype(jnp.bfloat16)
            blocks[first, :, low : low + 512] = part[:rows]
            blocks[first + 1, :, low : low + 512] = part[rows:]

    project(attended, 0)
    flip.wait()
    project(upper_recv, 2)

    def relay_copy(way):
        return remote(
            blocks.at[opposite, pl.ds(way * half, half), :], relayed.at[way],
            relay_send.at[way], relay_recv.at[way], devices[way],
        )

    def y_copy(way, part, source):
        return remote(
            source, arrived.at[way, pl.ds(part * half, half), :],
            y_send.at[way, part], y_recv.at[way, part], devices[way],
        )

    for way in range(2):
        relay_copy(way).start()
    for way in range(2):
        source = blocks.at[(after, before)[way], pl.ds((1 - way) * half, half), :]
        y_copy(way, 1 - way, source).start()
    for way in range(2):
        relay_copy(way).wait_recv()
        mine = blocks[(after, before)[way], way * half : (way + 1) * half, :]
        totals[way] = (
            mine.astype(jnp.float32) + relayed[way].astype(jnp.float32)
        ).astype(jnp.bfloat16)
        y_copy(way, way, totals.at[way]).start()
    for way in range(2):
        for part in range(2):
            copy = y_copy(way, part, totals.at[way])
            copy.wait_recv()
            copy.wait_send()
        relay_copy(way).wait_send()
    out_ref[...] = (
        blocks[t].astype(jnp.float32)
        + arrived[0].astype(jnp.float32)
        + arrived[1].astype(jnp.float32)
    ).astype(jnp.bfloat16)


def mixer_call(head_lambda, sub_gain, partial, parts, out_weight):
    dma = pltpu.SemaphoreType.DMA
    rows, width = BLOCK // NT, out_weight.shape[1]
    return pl.pallas_call(
        mixer_kernel,
        out_shape=jax.ShapeDtypeStruct((rows, width), jnp.bfloat16),
        in_specs=[pl.BlockSpec(memory_space=pltpu.SMEM)] + [VMEM] * 4,
        out_specs=VMEM,
        scratch_shapes=[
            pltpu.VMEM((BLOCK, HALF), jnp.bfloat16),
            pltpu.VMEM((BLOCK, HALF), jnp.bfloat16),
            pltpu.VMEM((BLOCK, HALF), jnp.bfloat16),
            pltpu.VMEM((NT, rows, width), jnp.bfloat16),
            pltpu.VMEM((2, rows // 2, width), jnp.bfloat16),
            pltpu.VMEM((2, rows // 2, width), jnp.bfloat16),
            pltpu.VMEM((2, rows, width), jnp.bfloat16),
            dma(()), dma(()), dma((2,)), dma((2,)), dma((2, 2)), dma((2, 2)),
        ],
        compiler_params=pltpu.CompilerParams(
            collective_id=2, has_side_effects=True, vmem_limit_bytes=24 * 2**20
        ),
        name="mixer",
    )(head_lambda, sub_gain[:, None], partial, parts, out_weight)


def shards(
    queries,
    key_rows,
    value_rows,
    head_lambda,
    sub_gain,
    out_weight,
    expert_input,
    norm_gain,
    route_ids,
    route_weight,
    gate_weight,
    up_weight,
    down_weight,
):
    rows_here, model_width = expert_input.shape
    experts = NZ * NX * NC
    top_count = route_ids.shape[1]
    slots = experts * (FULL + TAIL)
    wide_rows = expert_input.astype(jnp.float32)
    normed = (
        wide_rows
        * lax.rsqrt(jnp.mean(wide_rows * wide_rows, axis=-1, keepdims=True) + EPS)
        * norm_gain
    ).astype(jnp.bfloat16)
    flat_ids = route_ids.reshape(-1)
    onehot = (flat_ids[:, None] == jnp.arange(experts, dtype=jnp.int32)[None, :]).astype(jnp.int32)
    rank_before = jnp.cumsum(onehot, axis=0) - onehot
    slot = jnp.sum(rank_before * onehot, axis=1)
    buffer_pos = jnp.where(
        slot < FULL,
        flat_ids * FULL + slot,
        experts * FULL + flat_ids * TAIL + slot - FULL,
    ).reshape(rows_here, top_count)
    matches = buffer_pos[None, :, :] == jnp.arange(slots, dtype=jnp.int32)[:, None, None]
    dispatch = jnp.any(matches, axis=-1).astype(jnp.bfloat16)
    combine = jnp.sum(jnp.where(matches, route_weight[None, :, :], 0.0), axis=-1)
    own_cols = lax.dynamic_slice_in_dim(normed, lax.axis_index("tp") * COLS_T, COLS_T, 1)
    outgoing = jnp.dot(dispatch, own_cols, preferred_element_type=jnp.float32).astype(jnp.bfloat16)
    main = outgoing[: experts * FULL].reshape(experts, FULL, COLS_T)
    tail = outgoing[experts * FULL :].reshape(experts, TAIL, COLS_T)
    pair = jnp.concatenate([key_rows, value_rows.T], axis=0)
    turned = queries.T
    halves = jnp.stack([turned[:, :HALF], turned[:, HALF:]])

    xmain, xtail, pairs, parts = dispatch_call(main, tail, pair, halves)
    fmain, ftail = hidden_call(
        xmain.reshape(experts * FULL, model_width),
        xtail.reshape(experts * TAIL, model_width),
        gate_weight[0],
        up_weight[0],
        down_weight[0],
    )
    partial = flash(parts, pairs)
    rmain, rtail, others = return_call(
        fmain.reshape(experts, FULL, model_width),
        ftail.reshape(experts, TAIL, model_width),
        partial,
    )
    mixer_out = mixer_call(head_lambda, sub_gain, partial, others, out_weight)
    returned = jnp.concatenate(
        [rmain.reshape(experts * FULL, COLS_T), rtail.reshape(experts * TAIL, COLS_T)], axis=0
    )
    mixed = lax.dot_general(
        combine,
        returned.astype(jnp.float32),
        (((0,), (0,)), ((), ())),
        preferred_element_type=jnp.float32,
    )
    return (mixer_out, mixed.astype(jnp.bfloat16))


def solution(mesh):
    mesh = Mesh(mesh.devices.reshape(NZ, NX, NC, NT), (*EP, "tp"))
    placed = (
        P(EP, "tp"),
        P(EP, "tp"),
        P(EP, "tp"),
        P("tp"),
        P(),
        P("tp", None),
        P(EP, None),
        P(),
        P(EP, None),
        P(EP, None),
        P(EP, None, "tp"),
        P(EP, None, "tp"),
        P(EP, "tp", None),
    )
    return jax.shard_map(
        shards,
        mesh=mesh,
        in_specs=placed,
        out_specs=(P((*EP, "tp"), None), P(EP, "tp")),
        check_vma=False,
    )
```

```python
import functools
import math

import jax
import jax.numpy as jnp
from jax import lax
from jax.experimental import pallas as pl
from jax.experimental.pallas import tpu as pltpu
from jax.sharding import Mesh, PartitionSpec as P

EPS = 1e-06
NZ, NX, NC, NT = 8, 4, 2, 4
EP = ("z", "x", "core")
BLOCK = 256
HALF = BLOCK // 2
CHUNK = NC * BLOCK
COLS = 2 * NX * HALF
ACC = 144
COLS_T = 512
FULL, TAIL = 8, 2
NEAR = (0, 1, 7, 2, 6, 3, 5, 4)
PLUS = (0, 7, 6, 5)
LOW = -1e30
EXP2_SCALE = 64 ** (-0.5) * math.log2(math.e)


def pieces_of(value):
    first = value.astype(jnp.bfloat16).astype(jnp.float32)
    second = (value - first).astype(jnp.bfloat16).astype(jnp.float32)
    third = value - first - second
    return first, second, third


def places():
    return tuple(lax.axis_index(name) for name in (*EP, "tp"))


def remote(source, target, send, receive, device):
    return pltpu.make_async_remote_copy(
        src_ref=source,
        dst_ref=target,
        send_sem=send,
        recv_sem=receive,
        device_id=device,
        device_id_type=pl.DeviceIdType.MESH,
    )


def greet_all(z, x, c, t):
    me = (z * NX + x) * NC + c
    barrier = pltpu.get_barrier_semaphore()

    def signal(step, carry):
        peer = lax.rem(me + step, NZ * NX * NC)
        device = (peer // (NX * NC), lax.rem(peer // NC, NX), lax.rem(peer, NC), t)
        pl.semaphore_signal(
            barrier, inc=1, device_id=device, device_id_type=pl.DeviceIdType.MESH
        )
        return carry

    for dy in (1, NT - 1):
        pl.semaphore_signal(
            barrier,
            inc=1,
            device_id=(z, x, c, lax.rem(t + dy, NT)),
            device_id_type=pl.DeviceIdType.MESH,
        )
    lax.fori_loop(1, NZ * NX * NC, signal, 0)
    pl.semaphore_wait(barrier, NZ * NX * NC + 1)


def columns_of(t):
    return pl.ds(pl.multiple_of(t * COLS_T, COLS_T), COLS_T)


def dispatch_kernel(
    main_ref, tail_ref, pair_ref, query_ref, gate_ref, up_ref, down_ref,
    fmain, ftail, pairs, parts, xmain, xtail, taken, hidden, gate, up, down,
    w_sem, own_sem, out_send, out_recv, y_send, y_recv, kv_send, kv_recv, c_send, c_recv, q_send, q_recv,
):
    z, x, c, t = places()
    me = (z * NX + x) * NC + c
    local = x * NC + c
    group = NX * NC
    after, before = lax.rem(t + 1, NT), lax.rem(t + NT - 1, NT)
    own = columns_of(t)
    own_copies = [
        pltpu.make_async_copy(main_ref.at[me], xmain.at[me, :, own], own_sem.at[0]),
        pltpu.make_async_copy(tail_ref.at[me], xtail.at[me, :, own], own_sem.at[1]),
        pltpu.make_async_copy(pair_ref, pairs.at[z * NC + c], own_sem.at[2]),
        pltpu.make_async_copy(query_ref.at[0], parts.at[0, 0], own_sem.at[3]),
    ]
    weight_copies = [
        pltpu.make_async_copy(source, target, w_sem.at[k])
        for k, (source, target) in enumerate(((gate_ref, gate), (up_ref, up), (down_ref, down)))
    ]
    for copy in own_copies + weight_copies:
        copy.start()
    greet_all(z, x, c, t)

    for dz in (1, 7, 2, 6, 3, 5, 4, 0):
        to_z = lax.rem(z + dz, NZ)

        def send(step, carry):
            peer = lax.rem(local + step, group)
            device = (to_z, peer // NC, lax.rem(peer, NC), t)
            slab = to_z * group + peer
            for k, (source, target) in enumerate(((main_ref, xmain), (tail_ref, xtail))):
                remote(
                    source.at[slab], target.at[me, :, own],
                    out_send.at[k], out_recv.at[k, dz], device,
                ).start()
            return carry

        lax.fori_loop(1 if dz == 0 else 0, group, send, 0)

    mirrored = (NZ - 1 - z, x, c, t)
    remote(query_ref.at[1], parts.at[1, 0], q_send.at[3], q_recv.at[3], mirrored).start()
    for k in range(1, NX):
        device = (z, lax.rem(x + k, NX), c, t)
        remote(query_ref.at[0], parts.at[0, k], q_send.at[k - 1], q_recv.at[k - 1], device).start()

    higher, lower = (lax.rem(z + 1, NZ), x, c, t), (lax.rem(z + NZ - 1, NZ), x, c, t)
    across = (z, x, 1 - c, t)
    for way, device in enumerate((higher, lower)):
        remote(
            pair_ref, pairs.at[z * NC + c], kv_send.at[way, 0], kv_recv.at[way, 0], device
        ).start()
    remote(pair_ref, pairs.at[z * NC + c], c_send.at[0], c_recv.at[0], across).start()

    def rows_of(dz):
        return pl.ds(lax.rem(z - dz + NZ, NZ) * group, group)

    def y_copies(dz, slot, columns, device):
        rows = rows_of(dz)
        return [
            remote(
                target.at[rows, :, columns], target.at[rows, :, columns],
                y_send.at[slot, dz, k], y_recv.at[slot, dz, k], device,
            )
            for k, target in enumerate((xmain, xtail))
        ]

    to_after, to_before = (z, x, c, after), (z, x, c, before)

    def y_relay(dz):
        first = y_copies(dz, 0 if dz in PLUS else 1, own, to_after)
        for copy in first:
            copy.wait_recv()
        if dz in PLUS:
            copies = y_copies(dz, 2, columns_of(before), to_after)
        else:
            copies = y_copies(dz, 2, columns_of(after), to_before)
        for copy in copies:
            copy.start()

    def kv_step(step):
        for way, device in enumerate((higher, lower)):
            back = NZ - step if way == 0 else step
            block = lax.rem(z + back, NZ) * NC + c
            if step < 4:
                here = pairs.at[block]
                onward = here
                if step == 3:
                    onward = pairs.at[block, pl.ds(way * BLOCK, BLOCK), :]
            else:
                here = pairs.at[block, pl.ds(way * BLOCK, BLOCK), :]
            remote(
                here, here, kv_send.at[way, step - 1], kv_recv.at[way, step - 1], device
            ).wait_recv()
            if step < 4:
                remote(
                    onward, onward, kv_send.at[way, step], kv_recv.at[way, step], device
                ).start()
            slot = 2 * step - 1 + way
            remote(here, here, c_send.at[slot], c_recv.at[slot], across).start()

    for copy in own_copies:
        copy.wait()
    for index, dz in enumerate(NEAR):
        count = group - 1 if dz == 0 else group
        first = 0 if dz == 0 else lax.rem(z - dz + NZ, NZ) * group
        rows = pl.ds(first, count)
        for k, (source, target) in enumerate(((main_ref, xmain), (tail_ref, xtail))):
            remote(
                source.at[pl.ds(0, count)], target.at[rows, :, own],
                out_send.at[k], out_recv.at[k, dz], higher,
            ).wait_recv()
        for slot, device in enumerate((to_after, to_before)):
            for copy in y_copies(dz, slot, own, device):
                copy.start()
        if index == 1:
            remote(
                query_ref.at[1], parts.at[1, 0], q_send.at[3], q_recv.at[3], mirrored
            ).wait_recv()
            for k in range(1, NX):
                device = (z, lax.rem(x + k, NX), c, t)
                remote(
                    parts.at[1, 0], parts.at[1, k], q_send.at[3 + k], q_recv.at[3 + k], device
                ).start()
        if index >= 2:
            y_relay(NEAR[index - 2])
    kv_step(1)
    y_relay(NEAR[6])
    y_relay(NEAR[7])
    kv_step(2)
    for dz in NEAR:
        for copy in y_copies(dz, 1 if dz in PLUS else 0, own, to_after):
            copy.wait_recv()
        for copy in y_copies(dz, 2, own, to_after):
            copy.wait_recv()
    for copy in weight_copies:
        copy.wait()
    slabs, width = NZ * group, hidden.shape[1]
    taken[0 : slabs * FULL] = xmain[...].reshape(slabs * FULL, NT * COLS_T)
    taken[slabs * FULL :] = xtail[...].reshape(slabs * TAIL, NT * COLS_T)
    for first in range(0, width, 256):
        cols = slice(first, min(first + 256, width))
        gate_act = jnp.dot(taken[...], gate[:, cols], preferred_element_type=jnp.float32)
        up_act = jnp.dot(taken[...], up[:, cols], preferred_element_type=jnp.float32)
        value = gate_act / (1.0 + jnp.exp(-gate_act)) * up_act
        hidden[:, cols] = value.astype(jnp.bfloat16)
        if first == 256:
            kv_step(3)
    for first in range(0, NT * COLS_T, 256):
        cols = slice(first, first + 256)
        out = jnp.dot(hidden[...], down[:, cols], preferred_element_type=jnp.float32)
        out = out.astype(jnp.bfloat16)
        fmain[:, :, cols] = out[: slabs * FULL].reshape(slabs, FULL, 256)
        ftail[:, :, cols] = out[slabs * FULL :].reshape(slabs, TAIL, 256)
    kv_step(4)

    for dz in NEAR:
        for slot in range(3):
            for copy in y_copies(dz, slot, own, to_after):
                copy.wait_send()
    for k, (source, target) in enumerate(((main_ref, xmain), (tail_ref, xtail))):
        every = pl.ds(0, NZ * group - 1)
        remote(
            source.at[every], target.at[every, :, own], out_send.at[k], out_recv.at[k, 0], higher
        ).wait_send()
    for way in range(2):
        for step in range(4):
            block = pairs.at[0] if step < 3 else pairs.at[0, pl.ds(0, BLOCK), :]
            remote(block, block, kv_send.at[way, step], kv_recv.at[way, step], higher).wait_send()
    for slot in range(9):
        block = pairs.at[0] if slot < 7 else pairs.at[0, pl.ds(0, BLOCK), :]
        copy = remote(block, block, c_send.at[slot], c_recv.at[slot], across)
        copy.wait_send()
        copy.wait_recv()
    for slot in range(7):
        copy = remote(parts.at[0, 0], parts.at[0, 0], q_send.at[slot], q_recv.at[slot], higher)
        copy.wait_send()
        if slot != 3:
            copy.wait_recv()


VMEM = pl.BlockSpec(memory_space=pltpu.VMEM)
HBM = pl.BlockSpec(memory_space=pl.ANY)


def dispatch_call(main, tail, pair, queries, gate, up, down):
    dma = pltpu.SemaphoreType.DMA
    slabs, width = NZ * NX * NC, NT * COLS_T
    units = gate.shape[1]
    return pl.pallas_call(
        dispatch_kernel,
        out_shape=(
            jax.ShapeDtypeStruct((slabs, FULL, width), jnp.bfloat16),
            jax.ShapeDtypeStruct((slabs, TAIL, width), jnp.bfloat16),
            jax.ShapeDtypeStruct((NZ * NC, 2 * BLOCK, BLOCK), jnp.bfloat16),
            jax.ShapeDtypeStruct((2, NX, BLOCK, HALF), jnp.bfloat16),
        ),
        in_specs=[VMEM] * 4 + [HBM] * 3,
        out_specs=(VMEM,) * 4,
        scratch_shapes=[
            pltpu.VMEM((slabs, FULL, width), jnp.bfloat16),
            pltpu.VMEM((slabs, TAIL, width), jnp.bfloat16),
            pltpu.VMEM((slabs * (FULL + TAIL), width), jnp.bfloat16),
            pltpu.VMEM((slabs * (FULL + TAIL), units), jnp.bfloat16),
            pltpu.VMEM((width, units), jnp.bfloat16),
            pltpu.VMEM((width, units), jnp.bfloat16),
            pltpu.VMEM((units, width), jnp.bfloat16),
            dma((3,)), dma((4,)), dma((2,)), dma((2, NZ)), dma((3, NZ, 2)), dma((3, NZ, 2)),
            dma((2, 4)), dma((2, 4)), dma((9,)), dma((9,)), dma((7,)), dma((7,)),
        ],
        compiler_params=pltpu.CompilerParams(
            collective_id=0, has_side_effects=True, vmem_limit_bytes=44 * 2**20
        ),
        name="dispatch",
    )(main, tail, pair, queries, gate, up, down)


def main_kernel(
    lambda_ref, gain_ref, fmain, ftail, query_ref, pair_ref, weight_ref,
    out_ref, rmain, rtail,
    rhs_ref, max_ref, acc_ref, partial, parts,
    attended, upper_send, upper_recv, blocks, relayed, totals, arrived_y,
    relay_main, relay_tail, sum_main, sum_tail, in_main, in_tail, red_main, red_tail,
    own_sem, p_send, p_recv, relay_send, relay_recv, y_send, y_recv, out_send, out_recv,
    u_send, u_recv, mix_send, mix_recv, sum_send, sum_recv,
):
    z, x, c, t = places()
    me = (z * NX + x) * NC + c
    local = x * NC + c
    group = NX * NC
    after, before = lax.rem(t + 1, NT), lax.rem(t + NT - 1, NT)
    opposite = lax.rem(t + 2, NT)
    to_after, to_before = (z, x, c, after), (z, x, c, before)
    devices = (to_after, to_before)
    mirrored = (NZ - 1 - z, x, c, t)
    greet_all(z, x, c, t)
    far = NEAR[::-1]
    pairs = (
        (fmain, relay_main, sum_main, in_main, red_main, rmain),
        (ftail, relay_tail, sum_tail, in_tail, red_tail, rtail),
    )

    def rows_of(dz):
        return pl.ds(lax.rem(z + dz, NZ) * group, group)

    def relay_copy(dz, k):
        source, target = pairs[k][0], pairs[k][1]
        return remote(
            source.at[rows_of(dz), :, columns_of(opposite)], target.at[dz],
            relay_send.at[dz, k], relay_recv.at[dz, k],
            to_after if dz in PLUS else to_before,
        )

    def y_copy(dz, k, way, source):
        return remote(
            source, pairs[k][3].at[way, dz], y_send.at[way, dz, k], y_recv.at[way, dz, k],
            (to_after, to_before)[way],
        )

    def direct(dz, k):
        way = 1 if dz in PLUS else 0
        columns = columns_of((after, before)[way])
        return y_copy(dz, k, way, pairs[k][0].at[rows_of(dz), :, columns])

    for dz in far:
        for k in range(2):
            relay_copy(dz, k).start()
    for dz in far:
        for k in range(2):
            direct(dz, k).start()

    def add_relay(dz):
        way = 0 if dz in PLUS else 1
        columns = columns_of((after, before)[way])
        for k in range(2):
            relay_copy(dz, k).wait_recv()
            source, relayed, total = pairs[k][:3]
            mine = source[rows_of(dz), :, columns].astype(jnp.float32)
            total[dz] = (mine + relayed[dz].astype(jnp.float32)).astype(jnp.bfloat16)
            y_copy(dz, k, way, total.at[dz]).start()

    def finish(dz):
        to_z = lax.rem(z + dz, NZ)
        for k in range(2):
            source, arrived, reduced = pairs[k][0], pairs[k][3], pairs[k][4]
            for way in range(2):
                y_copy(dz, k, way, pairs[k][2].at[dz]).wait_recv()
            reduced[rows_of(dz)] = (
                source[rows_of(dz), :, columns_of(t)].astype(jnp.float32)
                + arrived[0, dz].astype(jnp.float32)
                + arrived[1, dz].astype(jnp.float32)
            ).astype(jnp.bfloat16)

        def send(step, carry):
            peer = lax.rem(local + step, group)
            device = (to_z, peer // NC, lax.rem(peer, NC), t)
            for k in range(2):
                remote(
                    pairs[k][4].at[to_z * group + peer], pairs[k][5].at[me],
                    out_send.at[k], out_recv.at[k], device,
                ).start()
            return carry

        lax.fori_loop(1 if dz == 0 else 0, group, send, 0)
        if dz == 0:
            for k in range(2):
                pltpu.make_async_copy(
                    pairs[k][4].at[me], pairs[k][5].at[me], own_sem.at[k]
                ).start()

    map_row = lax.broadcasted_iota(jnp.int32, (128, HALF), 0)
    for way in range(2):
        for head in range(2):
            for step in range(NX):
                block = query_ref[way, step, head * 128 : (head + 1) * 128, :]
                for which in range(2):
                    first = (which * NX + step) * HALF
                    keep = (map_row < 64) if which == 0 else (map_row >= 64)
                    rhs_ref[head, way, :, first : first + HALF] = jnp.where(
                        keep, block, jnp.zeros_like(block)
                    )
    max_ref[...] = jnp.full_like(max_ref, LOW)
    acc_ref[...] = jnp.zeros_like(acc_ref)
    ones = jnp.ones((ACC - 128, CHUNK), jnp.bfloat16)
    tile = 256
    units = NZ + 1

    def work(head, way, step_z, masked):
        lanes = pl.ds(pl.multiple_of(head * 128, 128), 128)
        below = pl.ds(pl.multiple_of(256 + head * 128, 128), 128)
        keys = [pair_ref[step_z * NC + k, 0:256, lanes] for k in range(NC)]
        values = [pair_ref[step_z * NC + k, below, :] for k in range(NC)]
        keys = jnp.concatenate(keys, axis=0)
        values = jnp.concatenate([jnp.concatenate(values, axis=1), ones], axis=0)
        for first in range(0, COLS, tile):
            cols = slice(first, first + tile)
            scores = jnp.dot(keys, rhs_ref[head, way, :, cols], preferred_element_type=jnp.float32)
            if masked:
                key = lax.broadcasted_iota(jnp.int32, (CHUNK, tile), 0) + 2 * BLOCK * x
                col = lax.broadcasted_iota(jnp.int32, (1, tile), 1) + first
                query_x = lax.rem(x - (col // HALF) % NX + NX, NX)
                position = (2 * query_x + c) * BLOCK + way * HALF + col % HALF
                scores = jnp.where(position >= key, scores, -3e38)
            earlier = max_ref[way, 0:1, cols]
            now = jnp.maximum(earlier, jnp.max(scores, axis=0, keepdims=True))
            weights = jnp.exp2((scores - now) * EXP2_SCALE).astype(jnp.bfloat16)
            rescale = jnp.exp2((earlier - now) * EXP2_SCALE)
            max_ref[way, 0:1, cols] = now
            acc_ref[way, :, cols] = acc_ref[way, :, cols] * rescale + jnp.dot(
                values, weights, preferred_element_type=jnp.float32
            )

    def x_copy(head, k):
        maps = pl.ds(2 * head, 2)
        device = (z, lax.rem(x + NX - k, NX), c, t)
        return remote(
            partial.at[k, maps], parts.at[k - 1, maps],
            p_send.at[head, k - 1], p_recv.at[head, k - 1], device,
        )

    def send_partial(head):
        row = lax.broadcasted_iota(jnp.int32, (ACC - 128, COLS), 0)
        for way in range(2):
            stats = jnp.zeros((ACC - 128, COLS), jnp.float32)
            pieces = pieces_of(acc_ref[way, 128:129, :]) + pieces_of(max_ref[way, 0:1, :])
            for index, piece in enumerate(pieces):
                stats = jnp.where(row == index, piece, stats)
            for which in range(2):
                for step in range(NX):
                    first = (which * NX + step) * HALF
                    lanes = slice(way * HALF, (way + 1) * HALF)
                    partial[step, 2 * head + which, 0:128, lanes] = acc_ref[
                        way, 0:128, first : first + HALF
                    ].astype(jnp.bfloat16)
                    partial[step, 2 * head + which, 128:ACC, lanes] = stats[
                        :, first : first + HALF
                    ].astype(jnp.bfloat16)
        for k in range(1, NX):
            x_copy(head, k).start()

    def unit(index, carry):
        head = index // units
        step = lax.rem(index, units)
        way = jnp.where(step > z, 1, 0)
        step_z = jnp.where(step > z, step - z - 1, step)
        last = (step == z) | (step == units - 1)

        @pl.when(last)
        def _():
            work(head, way, step_z, True)

        @pl.when(jnp.logical_not(last))
        def _():
            work(head, way, step_z, False)

        for k, dz in enumerate(far):

            @pl.when(index == 2 * k)
            def _():
                add_relay(dz)

            @pl.when(index == 2 * k + 2)
            def _():
                finish(dz)

        @pl.when(index == units - 1)
        def _():
            send_partial(0)
            max_ref[...] = jnp.full_like(max_ref, LOW)
            acc_ref[...] = jnp.zeros_like(acc_ref)

        return carry

    lax.fori_loop(0, 2 * units, unit, 0)
    send_partial(1)

    for head in range(2):
        for k in range(1, NX):
            x_copy(head, k).wait_recv()
        per_map = []
        for which in range(2):
            index = 2 * head + which
            sources = [partial.at[0, index]] + [parts.at[k, index] for k in range(NX - 1)]
            totals_of, maxima = [], []
            for part in sources:
                stats = part[128:ACC, :].astype(jnp.float32)
                totals_of.append(stats[0:1] + stats[1:2] + stats[2:3])
                maxima.append(stats[3:4] + stats[4:5] + stats[5:6])
            largest = functools.reduce(jnp.maximum, maxima)
            total, numerator = 0.0, 0.0
            for part, own_total, own_max in zip(sources, totals_of, maxima):
                factor = jnp.exp2((own_max - largest) * EXP2_SCALE)
                total = total + factor * own_total
                numerator = numerator + factor * part[0:128, :].astype(jnp.float32)
            per_map.append(numerator / total)
        contrast = per_map[0] - lambda_ref[head] * per_map[1]
        square = jnp.mean(contrast * contrast, axis=0, keepdims=True)
        normed = contrast * lax.rsqrt(square + EPS) * gain_ref[...]
        normed = normed.astype(jnp.bfloat16)
        attended[head * 128 : (head + 1) * 128, :] = normed[:, :HALF]
        upper_send[head * 128 : (head + 1) * 128, :] = normed[:, HALF:]

    flip = remote(upper_send, upper_recv, u_send, u_recv, mirrored)
    flip.start()
    rows = BLOCK // NT
    half = rows // 2

    def project(source, first):
        for low in range(0, 2048, 512):
            part = lax.dot_general(
                source[...], weight_ref[:, low : low + 512],
                (((0,), (0,)), ((), ())), preferred_element_type=jnp.float32,
            ).astype(jnp.bfloat16)
            blocks[first, :, low : low + 512] = part[:rows]
            blocks[first + 1, :, low : low + 512] = part[rows:]

    project(attended, 0)
    flip.wait()
    project(upper_recv, 2)

    def mix_relay(way):
        return remote(
            blocks.at[opposite, pl.ds(way * half, half), :], relayed.at[way],
            mix_send.at[way], mix_recv.at[way], devices[way],
        )

    def mix_copy(way, part, source):
        return remote(
            source, arrived_y.at[way, pl.ds(part * half, half), :],
            sum_send.at[way, part], sum_recv.at[way, part], devices[way],
        )

    for way in range(2):
        mix_relay(way).start()
    for way in range(2):
        source = blocks.at[(after, before)[way], pl.ds((1 - way) * half, half), :]
        mix_copy(way, 1 - way, source).start()
    for way in range(2):
        mix_relay(way).wait_recv()
        mine = blocks[(after, before)[way], way * half : (way + 1) * half, :]
        totals[way] = (
            mine.astype(jnp.float32) + relayed[way].astype(jnp.float32)
        ).astype(jnp.bfloat16)
        mix_copy(way, way, totals.at[way]).start()
    for way in range(2):
        for part in range(2):
            copy = mix_copy(way, part, totals.at[way])
            copy.wait_recv()
            copy.wait_send()
        mix_relay(way).wait_send()
    out_ref[...] = (
        blocks[t].astype(jnp.float32)
        + arrived_y[0].astype(jnp.float32)
        + arrived_y[1].astype(jnp.float32)
    ).astype(jnp.bfloat16)

    for k in range(2):
        pltpu.make_async_copy(pairs[k][4].at[me], pairs[k][5].at[me], own_sem.at[k]).wait()
        every = pl.ds(0, NZ * group - 1)
        copy = remote(
            pairs[k][4].at[every], pairs[k][5].at[every], out_send.at[k], out_recv.at[k], to_after
        )
        copy.wait_recv()
        copy.wait_send()
        for dz in far:
            relay_copy(dz, k).wait_send()
            for way in range(2):
                y_copy(dz, k, way, pairs[k][2].at[dz]).wait_send()
    for head in range(2):
        for k in range(1, NX):
            x_copy(head, k).wait_send()


def main_call(head_lambda, sub_gain, fmain, ftail, queries, pairs, out_weight):
    dma = pltpu.SemaphoreType.DMA
    slabs = NZ * NX * NC
    group = NX * NC
    rows, width = BLOCK // NT, out_weight.shape[1]
    bf16, f32 = jnp.bfloat16, jnp.float32

    def both(*lead):
        return [pltpu.VMEM((*lead, count, COLS_T), bf16) for count in (FULL, TAIL)]

    return pl.pallas_call(
        main_kernel,
        out_shape=(
            jax.ShapeDtypeStruct((rows, width), bf16),
            jax.ShapeDtypeStruct((slabs, FULL, COLS_T), bf16),
            jax.ShapeDtypeStruct((slabs, TAIL, COLS_T), bf16),
        ),
        in_specs=[pl.BlockSpec(memory_space=pltpu.SMEM)] + [VMEM] * 6,
        out_specs=(VMEM,) * 3,
        scratch_shapes=[
            pltpu.VMEM((2, 2, 128, COLS), bf16),
            pltpu.VMEM((2, 8, COLS), f32),
            pltpu.VMEM((2, ACC, COLS), f32),
            pltpu.VMEM((NX, 4, ACC, BLOCK), bf16),
            pltpu.VMEM((NX - 1, 4, ACC, BLOCK), bf16),
            pltpu.VMEM((BLOCK, HALF), bf16),
            pltpu.VMEM((BLOCK, HALF), bf16),
            pltpu.VMEM((BLOCK, HALF), bf16),
            pltpu.VMEM((NT, rows, width), bf16),
            pltpu.VMEM((2, rows // 2, width), bf16),
            pltpu.VMEM((2, rows // 2, width), bf16),
            pltpu.VMEM((2, rows, width), bf16),
            *both(NZ, group), *both(NZ, group), *both(2, NZ, group), *both(slabs),
            dma((2,)), dma((2, 3)), dma((2, 3)), dma((NZ, 2)), dma((NZ, 2)),
            dma((2, NZ, 2)), dma((2, NZ, 2)), dma((2,)), dma((2,)),
            dma(()), dma(()), dma((2,)), dma((2,)), dma((2, 2)), dma((2, 2)),
        ],
        compiler_params=pltpu.CompilerParams(
            collective_id=1, has_side_effects=True, vmem_limit_bytes=44 * 2**20
        ),
        name="mixer",
    )(head_lambda, sub_gain[:, None], fmain, ftail, queries, pairs, out_weight)


def shards(
    queries,
    key_rows,
    value_rows,
    head_lambda,
    sub_gain,
    out_weight,
    expert_input,
    norm_gain,
    route_ids,
    route_weight,
    gate_weight,
    up_weight,
    down_weight,
):
    rows_here, model_width = expert_input.shape
    experts = NZ * NX * NC
    top_count = route_ids.shape[1]
    slots = experts * (FULL + TAIL)
    wide_rows = expert_input.astype(jnp.float32)
    normed = (
        wide_rows
        * lax.rsqrt(jnp.mean(wide_rows * wide_rows, axis=-1, keepdims=True) + EPS)
        * norm_gain
    ).astype(jnp.bfloat16)
    flat_ids = route_ids.reshape(-1)
    onehot = (flat_ids[:, None] == jnp.arange(experts, dtype=jnp.int32)[None, :]).astype(jnp.int32)
    rank_before = jnp.cumsum(onehot, axis=0) - onehot
    slot = jnp.sum(rank_before * onehot, axis=1)
    buffer_pos = jnp.where(
        slot < FULL,
        flat_ids * FULL + slot,
        experts * FULL + flat_ids * TAIL + slot - FULL,
    ).reshape(rows_here, top_count)
    matches = buffer_pos[None, :, :] == jnp.arange(slots, dtype=jnp.int32)[:, None, None]
    dispatch = jnp.any(matches, axis=-1).astype(jnp.bfloat16)
    combine = jnp.sum(jnp.where(matches, route_weight[None, :, :], 0.0), axis=-1)
    own_cols = lax.dynamic_slice_in_dim(normed, lax.axis_index("tp") * COLS_T, COLS_T, 1)
    outgoing = jnp.dot(dispatch, own_cols, preferred_element_type=jnp.float32).astype(jnp.bfloat16)
    main = outgoing[: experts * FULL].reshape(experts, FULL, COLS_T)
    tail = outgoing[experts * FULL :].reshape(experts, TAIL, COLS_T)
    pair = jnp.concatenate([key_rows, value_rows.T], axis=0)
    turned = queries.T
    halves = jnp.stack([turned[:, :HALF], turned[:, HALF:]])

    fmain, ftail, pairs, parts = dispatch_call(
        main, tail, pair, halves, gate_weight[0], up_weight[0], down_weight[0]
    )
    mixer_out, rmain, rtail = main_call(
        head_lambda, sub_gain, fmain, ftail, parts, pairs, out_weight
    )
    returned = jnp.concatenate(
        [rmain.reshape(experts * FULL, COLS_T), rtail.reshape(experts * TAIL, COLS_T)], axis=0
    )
    mixed = lax.dot_general(
        combine,
        returned.astype(jnp.float32),
        (((0,), (0,)), ((), ())),
        preferred_element_type=jnp.float32,
    )
    return (mixer_out, mixed.astype(jnp.bfloat16))


def solution(mesh):
    mesh = Mesh(mesh.devices.reshape(NZ, NX, NC, NT), (*EP, "tp"))
    placed = (
        P(EP, "tp"),
        P(EP, "tp"),
        P(EP, "tp"),
        P("tp"),
        P(),
        P("tp", None),
        P(EP, None),
        P(),
        P(EP, None),
        P(EP, None),
        P(EP, None, "tp"),
        P(EP, None, "tp"),
        P(EP, "tp", None),
    )
    return jax.shard_map(
        shards,
        mesh=mesh,
        in_specs=placed,
        out_specs=(P((*EP, "tp"), None), P(EP, "tp")),
        check_vma=False,
    )
```

```python
import functools
import math

import jax
import jax.numpy as jnp
from jax import lax
from jax.experimental import pallas as pl
from jax.experimental.pallas import tpu as pltpu
from jax.sharding import Mesh, PartitionSpec as P

EPS = 1e-06
NZ, NX, NC, NT = 8, 4, 2, 4
EP = ("z", "x", "core")
BLOCK = 256
HALF = BLOCK // 2
CHUNK = NC * BLOCK
COLS = 2 * NX * HALF
ACC = 144
COLS_T = 512
FULL, TAIL = 8, 2
NEAR = (0, 1, 7, 2, 6, 3, 5, 4)
PLUS = (0, 7, 6, 5)
LOW = -1e30
EXP2_SCALE = 64 ** (-0.5) * math.log2(math.e)


def pieces_of(value):
    first = value.astype(jnp.bfloat16).astype(jnp.float32)
    second = (value - first).astype(jnp.bfloat16).astype(jnp.float32)
    third = value - first - second
    return first, second, third


def places():
    return tuple(lax.axis_index(name) for name in (*EP, "tp"))


def remote(source, target, send, receive, device):
    return pltpu.make_async_remote_copy(
        src_ref=source,
        dst_ref=target,
        send_sem=send,
        recv_sem=receive,
        device_id=device,
        device_id_type=pl.DeviceIdType.MESH,
    )


def greet_all(z, x, c, t):
    me = (z * NX + x) * NC + c
    barrier = pltpu.get_barrier_semaphore()

    def signal(step, carry):
        peer = lax.rem(me + step, NZ * NX * NC)
        device = (peer // (NX * NC), lax.rem(peer // NC, NX), lax.rem(peer, NC), t)
        pl.semaphore_signal(
            barrier, inc=1, device_id=device, device_id_type=pl.DeviceIdType.MESH
        )
        return carry

    for dy in (1, NT - 1):
        pl.semaphore_signal(
            barrier,
            inc=1,
            device_id=(z, x, c, lax.rem(t + dy, NT)),
            device_id_type=pl.DeviceIdType.MESH,
        )
    lax.fori_loop(1, NZ * NX * NC, signal, 0)
    pl.semaphore_wait(barrier, NZ * NX * NC + 1)


def columns_of(t):
    return pl.ds(pl.multiple_of(t * COLS_T, COLS_T), COLS_T)


def layer_kernel(
    lambda_ref, gain_ref, main_ref, tail_ref, pair_ref, query_ref, weight_ref,
    gate_ref, up_ref, down_ref,
    out_ref, rmain, rtail,
    xmain, xtail, taken, hidden, gate, up, down, fmain, ftail, pairs, parts,
    rhs_ref, score_ref, max_ref, acc_ref, partial, others,
    attended, upper_send, upper_recv, blocks, relayed, totals, arrived_y,
    relay_main, relay_tail, sum_main, sum_tail, in_main, in_tail, red_main, red_tail,
    w_sem, own_sem, out_send, out_recv, y_send, y_recv, kv_send, kv_recv, c_send, c_recv,
    q_send, q_recv, r_sem, p_send, p_recv, relay_send, relay_recv, s_send, s_recv,
    back_send, back_recv, u_send, u_recv, mix_send, mix_recv, sum_send, sum_recv,
):
    z, x, c, t = places()
    me = (z * NX + x) * NC + c
    local = x * NC + c
    group = NX * NC
    after, before = lax.rem(t + 1, NT), lax.rem(t + NT - 1, NT)
    own = columns_of(t)
    own_copies = [
        pltpu.make_async_copy(main_ref.at[me], xmain.at[me, :, own], own_sem.at[0]),
        pltpu.make_async_copy(tail_ref.at[me], xtail.at[me, :, own], own_sem.at[1]),
        pltpu.make_async_copy(pair_ref, pairs.at[z * NC + c], own_sem.at[2]),
        pltpu.make_async_copy(query_ref.at[0], parts.at[0, 0], own_sem.at[3]),
    ]
    weight_copies = [
        pltpu.make_async_copy(source, target, w_sem.at[k])
        for k, (source, target) in enumerate(((gate_ref, gate), (up_ref, up), (down_ref, down)))
    ]
    for copy in own_copies + weight_copies:
        copy.start()
    greet_all(z, x, c, t)

    for dz in (1, 7, 2, 6, 3, 5, 4, 0):
        to_z = lax.rem(z + dz, NZ)

        def send(step, carry):
            peer = lax.rem(local + step, group)
            device = (to_z, peer // NC, lax.rem(peer, NC), t)
            slab = to_z * group + peer
            for k, (source, target) in enumerate(((main_ref, xmain), (tail_ref, xtail))):
                remote(
                    source.at[slab], target.at[me, :, own],
                    out_send.at[k], out_recv.at[k, dz], device,
                ).start()
            return carry

        lax.fori_loop(1 if dz == 0 else 0, group, send, 0)

    mirrored = (NZ - 1 - z, x, c, t)
    remote(query_ref.at[1], parts.at[1, 0], q_send.at[3], q_recv.at[3], mirrored).start()
    for k in range(1, NX):
        device = (z, lax.rem(x + k, NX), c, t)
        remote(query_ref.at[0], parts.at[0, k], q_send.at[k - 1], q_recv.at[k - 1], device).start()

    higher, lower = (lax.rem(z + 1, NZ), x, c, t), (lax.rem(z + NZ - 1, NZ), x, c, t)
    across = (z, x, 1 - c, t)
    for way, device in enumerate((higher, lower)):
        remote(
            pair_ref, pairs.at[z * NC + c], kv_send.at[way, 0], kv_recv.at[way, 0], device
        ).start()
    remote(pair_ref, pairs.at[z * NC + c], c_send.at[0], c_recv.at[0], across).start()

    def rows_of(dz):
        return pl.ds(lax.rem(z - dz + NZ, NZ) * group, group)

    def y_copies(dz, slot, columns, device):
        rows = rows_of(dz)
        return [
            remote(
                target.at[rows, :, columns], target.at[rows, :, columns],
                y_send.at[slot, dz, k], y_recv.at[slot, dz, k], device,
            )
            for k, target in enumerate((xmain, xtail))
        ]

    to_after, to_before = (z, x, c, after), (z, x, c, before)

    def y_relay(dz):
        first = y_copies(dz, 0 if dz in PLUS else 1, own, to_after)
        for copy in first:
            copy.wait_recv()
        if dz in PLUS:
            copies = y_copies(dz, 2, columns_of(before), to_after)
        else:
            copies = y_copies(dz, 2, columns_of(after), to_before)
        for copy in copies:
            copy.start()

    def kv_step(step):
        for way, device in enumerate((higher, lower)):
            back = NZ - step if way == 0 else step
            block = lax.rem(z + back, NZ) * NC + c
            if step < 4:
                here = pairs.at[block]
                onward = here
                if step == 3:
                    onward = pairs.at[block, pl.ds(way * BLOCK, BLOCK), :]
            else:
                here = pairs.at[block, pl.ds(way * BLOCK, BLOCK), :]
            remote(
                here, here, kv_send.at[way, step - 1], kv_recv.at[way, step - 1], device
            ).wait_recv()
            if step < 4:
                remote(
                    onward, onward, kv_send.at[way, step], kv_recv.at[way, step], device
                ).start()
            slot = 2 * step - 1 + way
            remote(here, here, c_send.at[slot], c_recv.at[slot], across).start()

    opposite = lax.rem(t + 2, NT)
    devices = (to_after, to_before)
    far = NEAR[::-1]
    stages = (
        (fmain, relay_main, sum_main, in_main, red_main, rmain),
        (ftail, relay_tail, sum_tail, in_tail, red_tail, rtail),
    )

    def back_rows(dz):
        return pl.ds(lax.rem(z + dz, NZ) * group, group)

    def relay_copy(dz, k):
        source, target = stages[k][0], stages[k][1]
        return remote(
            source.at[back_rows(dz), :, columns_of(opposite)], target.at[dz],
            relay_send.at[dz, k], relay_recv.at[dz, k],
            to_after if dz in PLUS else to_before,
        )

    def s_copy(dz, k, way, source):
        return remote(
            source, stages[k][3].at[way, dz], s_send.at[way, dz, k], s_recv.at[way, dz, k],
            (to_after, to_before)[way],
        )

    def direct(dz, k):
        way = 1 if dz in PLUS else 0
        columns = columns_of((after, before)[way])
        return s_copy(dz, k, way, stages[k][0].at[back_rows(dz), :, columns])

    for copy in own_copies:
        copy.wait()
    for index, dz in enumerate(NEAR):
        count = group - 1 if dz == 0 else group
        first = 0 if dz == 0 else lax.rem(z - dz + NZ, NZ) * group
        rows = pl.ds(first, count)
        for k, (source, target) in enumerate(((main_ref, xmain), (tail_ref, xtail))):
            remote(
                source.at[pl.ds(0, count)], target.at[rows, :, own],
                out_send.at[k], out_recv.at[k, dz], higher,
            ).wait_recv()
        for slot, device in enumerate((to_after, to_before)):
            for copy in y_copies(dz, slot, own, device):
                copy.start()
        if index == 1:
            remote(
                query_ref.at[1], parts.at[1, 0], q_send.at[3], q_recv.at[3], mirrored
            ).wait_recv()
            for k in range(1, NX):
                device = (z, lax.rem(x + k, NX), c, t)
                remote(
                    parts.at[1, 0], parts.at[1, k], q_send.at[3 + k], q_recv.at[3 + k], device
                ).start()
        if index >= 2:
            y_relay(NEAR[index - 2])
    kv_step(1)
    y_relay(NEAR[6])
    y_relay(NEAR[7])
    kv_step(2)
    for dz in NEAR:
        for copy in y_copies(dz, 1 if dz in PLUS else 0, own, to_after):
            copy.wait_recv()
        for copy in y_copies(dz, 2, own, to_after):
            copy.wait_recv()
    for copy in weight_copies:
        copy.wait()
    slabs, width = NZ * group, hidden.shape[1]
    taken[0 : slabs * FULL] = xmain[...].reshape(slabs * FULL, NT * COLS_T)
    taken[slabs * FULL :] = xtail[...].reshape(slabs * TAIL, NT * COLS_T)
    for first in range(0, width, 256):
        cols = slice(first, min(first + 256, width))
        gate_act = jnp.dot(taken[...], gate[:, cols], preferred_element_type=jnp.float32)
        up_act = jnp.dot(taken[...], up[:, cols], preferred_element_type=jnp.float32)
        value = gate_act / (1.0 + jnp.exp(-gate_act)) * up_act
        hidden[:, cols] = value.astype(jnp.bfloat16)
    for turn in (2, 1, 3, 0):
        for part in range(2):
            start = lax.rem(t + turn, NT) * COLS_T + part * 256
            cols = pl.ds(pl.multiple_of(start, 256), 256)
            out = jnp.dot(hidden[...], down[:, cols], preferred_element_type=jnp.float32)
            out = out.astype(jnp.bfloat16)
            fmain[:, :, cols] = out[: slabs * FULL].reshape(slabs, FULL, 256)
            ftail[:, :, cols] = out[slabs * FULL :].reshape(slabs, TAIL, 256)
        for dz in far:
            for k in range(2):
                if turn == 2:
                    relay_copy(dz, k).start()
                elif turn == (3 if dz in PLUS else 1):
                    direct(dz, k).start()
    kv_step(3)
    def add_relay(dz):
        way = 0 if dz in PLUS else 1
        columns = columns_of((after, before)[way])
        for k in range(2):
            relay_copy(dz, k).wait_recv()
            source, relayed, total = stages[k][:3]
            mine = source[back_rows(dz), :, columns].astype(jnp.float32)
            total[dz] = (mine + relayed[dz].astype(jnp.float32)).astype(jnp.bfloat16)
            s_copy(dz, k, way, total.at[dz]).start()

    def finish(dz):
        to_z = lax.rem(z + dz, NZ)
        for k in range(2):
            source, arrived, reduced = stages[k][0], stages[k][3], stages[k][4]
            for way in range(2):
                s_copy(dz, k, way, stages[k][2].at[dz]).wait_recv()
            reduced[back_rows(dz)] = (
                source[back_rows(dz), :, columns_of(t)].astype(jnp.float32)
                + arrived[0, dz].astype(jnp.float32)
                + arrived[1, dz].astype(jnp.float32)
            ).astype(jnp.bfloat16)

        def send(step, carry):
            peer = lax.rem(local + step, group)
            device = (to_z, peer // NC, lax.rem(peer, NC), t)
            for k in range(2):
                remote(
                    stages[k][4].at[to_z * group + peer], stages[k][5].at[me],
                    back_send.at[k], back_recv.at[k], device,
                ).start()
            return carry

        lax.fori_loop(1 if dz == 0 else 0, group, send, 0)
        if dz == 0:
            for k in range(2):
                pltpu.make_async_copy(
                    stages[k][4].at[me], stages[k][5].at[me], r_sem.at[k]
                ).start()

    for slot in range(7):
        if slot != 3:
            remote(
                parts.at[0, 0], parts.at[0, 0], q_send.at[slot], q_recv.at[slot], higher
            ).wait_recv()
    map_row = lax.broadcasted_iota(jnp.int32, (128, HALF), 0)
    for way in range(2):
        for head in range(2):
            for step in range(NX):
                block = parts[way, step, head * 128 : (head + 1) * 128, :]
                for which in range(2):
                    first = (which * NX + step) * HALF
                    keep = (map_row < 64) if which == 0 else (map_row >= 64)
                    rhs_ref[head, way, :, first : first + HALF] = jnp.where(
                        keep, block, jnp.zeros_like(block)
                    )
    max_ref[...] = jnp.full_like(max_ref, LOW)
    acc_ref[...] = jnp.zeros_like(acc_ref)
    ones = jnp.ones((ACC - 128, CHUNK), jnp.bfloat16)
    tile = 256
    turns = 2 * NZ

    def work(head, way, step_z, masked):
        lanes = pl.ds(pl.multiple_of(head * 128, 128), 128)
        below = pl.ds(pl.multiple_of(256 + head * 128, 128), 128)
        keys = [pairs[step_z * NC + k, 0:256, lanes] for k in range(NC)]
        values = [pairs[step_z * NC + k, below, :] for k in range(NC)]
        keys = jnp.concatenate(keys, axis=0)
        values = jnp.concatenate([jnp.concatenate(values, axis=1), ones], axis=0)

        def score(slot, first):
            cols = slice(first, first + tile)
            scores = jnp.dot(keys, rhs_ref[head, way, :, cols], preferred_element_type=jnp.float32)
            if masked:
                key = lax.broadcasted_iota(jnp.int32, (CHUNK, tile), 0) + 2 * BLOCK * x
                col = lax.broadcasted_iota(jnp.int32, (1, tile), 1) + first
                query_x = lax.rem(x - (col // HALF) % NX + NX, NX)
                position = (2 * query_x + c) * BLOCK + way * HALF + col % HALF
                scores = jnp.where(position >= key, scores, -3e38)
            score_ref[slot] = scores

        score(0, 0)
        for number in range(COLS // tile):
            first = number * tile
            if first + tile < COLS:
                score((number + 1) % 2, first + tile)
            scores = score_ref[number % 2]
            cols = slice(first, first + tile)
            earlier = max_ref[way, 0:1, cols]
            now = jnp.maximum(earlier, jnp.max(scores, axis=0, keepdims=True))
            weights = jnp.exp2((scores - now) * EXP2_SCALE).astype(jnp.bfloat16)
            rescale = jnp.exp2((earlier - now) * EXP2_SCALE)
            max_ref[way, 0:1, cols] = now
            acc_ref[way, :, cols] = acc_ref[way, :, cols] * rescale + jnp.dot(
                values, weights, preferred_element_type=jnp.float32
            )

    def x_copy(head, k):
        maps = pl.ds(2 * head, 2)
        device = (z, lax.rem(x + NX - k, NX), c, t)
        return remote(
            partial.at[k, maps], others.at[k - 1, maps],
            p_send.at[head, k - 1], p_recv.at[head, k - 1], device,
        )

    def send_partial(head):
        row = lax.broadcasted_iota(jnp.int32, (ACC - 128, COLS), 0)
        for way in range(2):
            stats = jnp.zeros((ACC - 128, COLS), jnp.float32)
            pieces = pieces_of(acc_ref[way, 128:129, :]) + pieces_of(max_ref[way, 0:1, :])
            for index, piece in enumerate(pieces):
                stats = jnp.where(row == index, piece, stats)
            for which in range(2):
                for step in range(NX):
                    first = (which * NX + step) * HALF
                    lanes = slice(way * HALF, (way + 1) * HALF)
                    partial[step, 2 * head + which, 0:128, lanes] = acc_ref[
                        way, 0:128, first : first + HALF
                    ].astype(jnp.bfloat16)
                    partial[step, 2 * head + which, 128:ACC, lanes] = stats[
                        :, first : first + HALF
                    ].astype(jnp.bfloat16)
        for k in range(1, NX):
            x_copy(head, k).start()

    def peer_copy(slot):
        block = pairs.at[0] if slot < 7 else pairs.at[0, pl.ds(0, BLOCK), :]
        return remote(block, block, c_send.at[slot], c_recv.at[slot], across)

    def unit(index, carry):
        head = index // turns
        turn = lax.rem(index, turns)
        way = lax.rem(turn, 2)
        near = turn // 2
        distance = (near + 1) // 2
        step_z = lax.rem(z + jnp.where(lax.rem(near, 2) == 1, NZ - distance, distance), NZ)
        query_z = jnp.where(way == 0, z, NZ - 1 - z)
        for place, slots in ((0, (0,)), (2, (1,)), (4, (2,)), (6, (3,)), (8, (4,)), (10, (5,)), (12, (6,)), (14, (7, 8))):

            @pl.when(index == place)
            def _():
                for slot in slots:
                    peer_copy(slot).wait_recv()

        @pl.when(step_z == query_z)
        def _():
            work(head, way, step_z, True)

        @pl.when(step_z < query_z)
        def _():
            work(head, way, step_z, False)

        for k, dz in enumerate(far):

            @pl.when(index == 2 * k)
            def _():
                add_relay(dz)

            @pl.when(index == 2 * k + 3)
            def _():
                finish(dz)

        @pl.when(index == 7)
        def _():
            kv_step(4)

        @pl.when(index == turns - 1)
        def _():
            send_partial(0)
            max_ref[...] = jnp.full_like(max_ref, LOW)
            acc_ref[...] = jnp.zeros_like(acc_ref)

        return carry

    lax.fori_loop(0, 2 * turns, unit, 0)
    send_partial(1)

    for head in range(2):
        for k in range(1, NX):
            x_copy(head, k).wait_recv()
        per_map = []
        for which in range(2):
            index = 2 * head + which
            sources = [partial.at[0, index]] + [others.at[k, index] for k in range(NX - 1)]
            totals_of, maxima = [], []
            for part in sources:
                stats = part[128:ACC, :].astype(jnp.float32)
                totals_of.append(stats[0:1] + stats[1:2] + stats[2:3])
                maxima.append(stats[3:4] + stats[4:5] + stats[5:6])
            largest = functools.reduce(jnp.maximum, maxima)
            total, numerator = 0.0, 0.0
            for part, own_total, own_max in zip(sources, totals_of, maxima):
                factor = jnp.exp2((own_max - largest) * EXP2_SCALE)
                total = total + factor * own_total
                numerator = numerator + factor * part[0:128, :].astype(jnp.float32)
            per_map.append(numerator / total)
        contrast = per_map[0] - lambda_ref[head] * per_map[1]
        square = jnp.mean(contrast * contrast, axis=0, keepdims=True)
        normed = contrast * lax.rsqrt(square + EPS) * gain_ref[...]
        normed = normed.astype(jnp.bfloat16)
        attended[head * 128 : (head + 1) * 128, :] = normed[:, :HALF]
        upper_send[head * 128 : (head + 1) * 128, :] = normed[:, HALF:]

    flip = remote(upper_send, upper_recv, u_send, u_recv, mirrored)
    flip.start()
    rows = BLOCK // NT
    half = rows // 2

    def project(source, first):
        for low in range(0, 2048, 512):
            part = lax.dot_general(
                source[...], weight_ref[:, low : low + 512],
                (((0,), (0,)), ((), ())), preferred_element_type=jnp.float32,
            ).astype(jnp.bfloat16)
            blocks[first, :, low : low + 512] = part[:rows]
            blocks[first + 1, :, low : low + 512] = part[rows:]

    project(attended, 0)
    flip.wait()
    project(upper_recv, 2)

    def mix_relay(way):
        return remote(
            blocks.at[opposite, pl.ds(way * half, half), :], relayed.at[way],
            mix_send.at[way], mix_recv.at[way], devices[way],
        )

    def mix_copy(way, part, source):
        return remote(
            source, arrived_y.at[way, pl.ds(part * half, half), :],
            sum_send.at[way, part], sum_recv.at[way, part], devices[way],
        )

    for way in range(2):
        mix_relay(way).start()
    for way in range(2):
        source = blocks.at[(after, before)[way], pl.ds((1 - way) * half, half), :]
        mix_copy(way, 1 - way, source).start()
    for way in range(2):
        mix_relay(way).wait_recv()
        mine = blocks[(after, before)[way], way * half : (way + 1) * half, :]
        totals[way] = (
            mine.astype(jnp.float32) + relayed[way].astype(jnp.float32)
        ).astype(jnp.bfloat16)
        mix_copy(way, way, totals.at[way]).start()
    for way in range(2):
        for part in range(2):
            copy = mix_copy(way, part, totals.at[way])
            copy.wait_recv()
            copy.wait_send()
        mix_relay(way).wait_send()
    out_ref[...] = (
        blocks[t].astype(jnp.float32)
        + arrived_y[0].astype(jnp.float32)
        + arrived_y[1].astype(jnp.float32)
    ).astype(jnp.bfloat16)

    for k in range(2):
        pltpu.make_async_copy(stages[k][4].at[me], stages[k][5].at[me], r_sem.at[k]).wait()
        every = pl.ds(0, NZ * group - 1)
        copy = remote(
            stages[k][4].at[every], stages[k][5].at[every], back_send.at[k], back_recv.at[k], to_after
        )
        copy.wait_recv()
        copy.wait_send()
        for dz in far:
            relay_copy(dz, k).wait_send()
            for way in range(2):
                s_copy(dz, k, way, stages[k][2].at[dz]).wait_send()
    for head in range(2):
        for k in range(1, NX):
            x_copy(head, k).wait_send()

    for dz in NEAR:
        for slot in range(3):
            for copy in y_copies(dz, slot, own, to_after):
                copy.wait_send()
    for k, (source, target) in enumerate(((main_ref, xmain), (tail_ref, xtail))):
        every = pl.ds(0, NZ * group - 1)
        remote(
            source.at[every], target.at[every, :, own], out_send.at[k], out_recv.at[k, 0], higher
        ).wait_send()
    for way in range(2):
        for step in range(4):
            block = pairs.at[0] if step < 3 else pairs.at[0, pl.ds(0, BLOCK), :]
            remote(block, block, kv_send.at[way, step], kv_recv.at[way, step], higher).wait_send()
    for slot in range(9):
        block = pairs.at[0] if slot < 7 else pairs.at[0, pl.ds(0, BLOCK), :]
        remote(block, block, c_send.at[slot], c_recv.at[slot], across).wait_send()
    for slot in range(7):
        remote(
            parts.at[0, 0], parts.at[0, 0], q_send.at[slot], q_recv.at[slot], higher
        ).wait_send()


VMEM = pl.BlockSpec(memory_space=pltpu.VMEM)
HBM = pl.BlockSpec(memory_space=pl.ANY)


def layer_call(head_lambda, sub_gain, main, tail, pair, queries, out_weight, gate, up, down):
    dma = pltpu.SemaphoreType.DMA
    slabs, group = NZ * NX * NC, NX * NC
    units = gate.shape[1]
    rows, width = BLOCK // NT, out_weight.shape[1]
    bf16, f32 = jnp.bfloat16, jnp.float32

    def both(*lead, columns=COLS_T):
        return [pltpu.VMEM((*lead, count, columns), bf16) for count in (FULL, TAIL)]

    return pl.pallas_call(
        layer_kernel,
        out_shape=(
            jax.ShapeDtypeStruct((rows, width), bf16),
            jax.ShapeDtypeStruct((slabs, FULL, COLS_T), bf16),
            jax.ShapeDtypeStruct((slabs, TAIL, COLS_T), bf16),
        ),
        in_specs=[pl.BlockSpec(memory_space=pltpu.SMEM)] + [VMEM] * 6 + [HBM] * 3,
        out_specs=(VMEM,) * 3,
        scratch_shapes=[
            *both(slabs, columns=width),
            pltpu.VMEM((slabs * (FULL + TAIL), width), bf16),
            pltpu.VMEM((slabs * (FULL + TAIL), units), bf16),
            pltpu.VMEM((width, units), bf16),
            pltpu.VMEM((width, units), bf16),
            pltpu.VMEM((units, width), bf16),
            *both(slabs, columns=width),
            pltpu.VMEM((NZ * NC, 2 * BLOCK, BLOCK), bf16),
            pltpu.VMEM((2, NX, BLOCK, HALF), bf16),
            pltpu.VMEM((2, 2, 128, COLS), bf16),
            pltpu.VMEM((2, CHUNK, 256), f32),
            pltpu.VMEM((2, 8, COLS), f32),
            pltpu.VMEM((2, ACC, COLS), f32),
            pltpu.VMEM((NX, 4, ACC, BLOCK), bf16),
            pltpu.VMEM((NX - 1, 4, ACC, BLOCK), bf16),
            pltpu.VMEM((BLOCK, HALF), bf16),
            pltpu.VMEM((BLOCK, HALF), bf16),
            pltpu.VMEM((BLOCK, HALF), bf16),
            pltpu.VMEM((NT, rows, width), bf16),
            pltpu.VMEM((2, rows // 2, width), bf16),
            pltpu.VMEM((2, rows // 2, width), bf16),
            pltpu.VMEM((2, rows, width), bf16),
            *both(NZ, group), *both(NZ, group), *both(2, NZ, group), *both(slabs),
            dma((3,)), dma((4,)), dma((2,)), dma((2, NZ)), dma((3, NZ, 2)), dma((3, NZ, 2)),
            dma((2, 4)), dma((2, 4)), dma((9,)), dma((9,)), dma((7,)), dma((7,)),
            dma((2,)), dma((2, 3)), dma((2, 3)), dma((NZ, 2)), dma((NZ, 2)),
            dma((2, NZ, 2)), dma((2, NZ, 2)), dma((2,)), dma((2,)),
            dma(()), dma(()), dma((2,)), dma((2,)), dma((2, 2)), dma((2, 2)),
        ],
        compiler_params=pltpu.CompilerParams(
            collective_id=0, has_side_effects=True, vmem_limit_bytes=56 * 2**20
        ),
        name="layer",
    )(head_lambda, sub_gain[:, None], main, tail, pair, queries, out_weight, gate, up, down)


def shards(
    queries,
    key_rows,
    value_rows,
    head_lambda,
    sub_gain,
    out_weight,
    expert_input,
    norm_gain,
    route_ids,
    route_weight,
    gate_weight,
    up_weight,
    down_weight,
):
    rows_here, model_width = expert_input.shape
    experts = NZ * NX * NC
    top_count = route_ids.shape[1]
    slots = experts * (FULL + TAIL)
    wide_rows = expert_input.astype(jnp.float32)
    normed = (
        wide_rows
        * lax.rsqrt(jnp.mean(wide_rows * wide_rows, axis=-1, keepdims=True) + EPS)
        * norm_gain
    ).astype(jnp.bfloat16)
    flat_ids = route_ids.reshape(-1)
    onehot = (flat_ids[:, None] == jnp.arange(experts, dtype=jnp.int32)[None, :]).astype(jnp.int32)
    rank_before = jnp.cumsum(onehot, axis=0) - onehot
    slot = jnp.sum(rank_before * onehot, axis=1)
    buffer_pos = jnp.where(
        slot < FULL,
        flat_ids * FULL + slot,
        experts * FULL + flat_ids * TAIL + slot - FULL,
    ).reshape(rows_here, top_count)
    matches = buffer_pos[None, :, :] == jnp.arange(slots, dtype=jnp.int32)[:, None, None]
    dispatch = jnp.any(matches, axis=-1).astype(jnp.bfloat16)
    combine = jnp.sum(jnp.where(matches, route_weight[None, :, :], 0.0), axis=-1)
    own_cols = lax.dynamic_slice_in_dim(normed, lax.axis_index("tp") * COLS_T, COLS_T, 1)
    outgoing = jnp.dot(dispatch, own_cols, preferred_element_type=jnp.float32).astype(jnp.bfloat16)
    main = outgoing[: experts * FULL].reshape(experts, FULL, COLS_T)
    tail = outgoing[experts * FULL :].reshape(experts, TAIL, COLS_T)
    pair = jnp.concatenate([key_rows, value_rows.T], axis=0)
    turned = queries.T
    halves = jnp.stack([turned[:, :HALF], turned[:, HALF:]])

    mixer_out, rmain, rtail = layer_call(
        head_lambda, sub_gain, main, tail, pair, halves, out_weight,
        gate_weight[0], up_weight[0], down_weight[0],
    )
    returned = jnp.concatenate(
        [rmain.reshape(experts * FULL, COLS_T), rtail.reshape(experts * TAIL, COLS_T)], axis=0
    )
    mixed = lax.dot_general(
        combine,
        returned.astype(jnp.float32),
        (((0,), (0,)), ((), ())),
        preferred_element_type=jnp.float32,
    )
    return (mixer_out, mixed.astype(jnp.bfloat16))


def solution(mesh):
    mesh = Mesh(mesh.devices.reshape(NZ, NX, NC, NT), (*EP, "tp"))
    placed = (
        P(EP, "tp"),
        P(EP, "tp"),
        P(EP, "tp"),
        P("tp"),
        P(),
        P("tp", None),
        P(EP, None),
        P(),
        P(EP, None),
        P(EP, None),
        P(EP, None, "tp"),
        P(EP, None, "tp"),
        P(EP, "tp", None),
    )
    return jax.shard_map(
        shards,
        mesh=mesh,
        in_specs=placed,
        out_specs=(P((*EP, "tp"), None), P(EP, "tp")),
        check_vma=False,
    )
```

```python
import functools
import math

import jax
import jax.numpy as jnp
from jax import lax
from jax.experimental import pallas as pl
from jax.experimental.pallas import tpu as pltpu
from jax.sharding import Mesh, PartitionSpec as P

EPS = 1e-06
NZ, NX, NC, NT = 8, 4, 2, 4
EP = ("z", "x", "core")
BLOCK = 256
HALF = BLOCK // 2
CHUNK = NC * BLOCK
COLS = 2 * NX * HALF
ACC = 144
COLS_T = 512
FULL, TAIL = 8, 2
NEAR = (0, 1, 7, 2, 6, 3, 5, 4)
PLUS = (0, 7, 6, 5)
LOW = -1e30
EXP2_SCALE = 64 ** (-0.5) * math.log2(math.e)


def pieces_of(value):
    first = value.astype(jnp.bfloat16).astype(jnp.float32)
    second = (value - first).astype(jnp.bfloat16).astype(jnp.float32)
    third = value - first - second
    return first, second, third


def places():
    return tuple(lax.axis_index(name) for name in (*EP, "tp"))


def remote(source, target, send, receive, device):
    return pltpu.make_async_remote_copy(
        src_ref=source,
        dst_ref=target,
        send_sem=send,
        recv_sem=receive,
        device_id=device,
        device_id_type=pl.DeviceIdType.MESH,
    )


def greet_all(z, x, c, t):
    me = (z * NX + x) * NC + c
    barrier = pltpu.get_barrier_semaphore()

    def signal(step, carry):
        peer = lax.rem(me + step, NZ * NX * NC)
        device = (peer // (NX * NC), lax.rem(peer // NC, NX), lax.rem(peer, NC), t)
        pl.semaphore_signal(
            barrier, inc=1, device_id=device, device_id_type=pl.DeviceIdType.MESH
        )
        return carry

    for dy in (1, NT - 1):
        pl.semaphore_signal(
            barrier,
            inc=1,
            device_id=(z, x, c, lax.rem(t + dy, NT)),
            device_id_type=pl.DeviceIdType.MESH,
        )
    lax.fori_loop(1, NZ * NX * NC, signal, 0)
    return barrier


def columns_of(t):
    return pl.ds(pl.multiple_of(t * COLS_T, COLS_T), COLS_T)


def layer_kernel(
    lambda_ref, gain_ref, keys_ref, values_ref, queries_ref, token_ref, norm_ref, ids_ref,
    share_ref, weight_ref, gate_ref, up_ref, down_ref,
    out_ref, mixed_ref,
    main_ref, tail_ref, pair_ref, query_ref, combine_ref, rmain, rtail,
    xmain, xtail, taken, hidden, gate, up, down, fmain, ftail, pairs, parts,
    rhs_ref, score_ref, max_ref, acc_ref, partial, others,
    attended, upper_send, upper_recv, blocks, relayed, totals, arrived_y,
    relay_main, relay_tail, sum_main, sum_tail, in_main, in_tail, red_main, red_tail,
    w_sem, own_sem, out_send, out_recv, y_send, y_recv, kv_send, kv_recv, c_send, c_recv,
    q_send, q_recv, r_sem, p_send, p_recv, relay_send, relay_recv, s_send, s_recv,
    back_send, back_recv, u_send, u_recv, mix_send, mix_recv, sum_send, sum_recv,
):
    z, x, c, t = places()
    me = (z * NX + x) * NC + c
    local = x * NC + c
    group = NX * NC
    after, before = lax.rem(t + 1, NT), lax.rem(t + NT - 1, NT)
    own = columns_of(t)
    weight_copies = [
        pltpu.make_async_copy(source, target, w_sem.at[k])
        for k, (source, target) in enumerate(((gate_ref, gate), (up_ref, up), (down_ref, down)))
    ]
    for copy in weight_copies:
        copy.start()
    barrier = greet_all(z, x, c, t)

    wide = token_ref[...].astype(jnp.float32)
    scale = lax.rsqrt(jnp.mean(wide * wide, axis=-1, keepdims=True) + EPS)
    normed_own = token_ref[:, own].astype(jnp.float32) * scale * norm_ref[:, own]
    normed_own = normed_own.astype(jnp.bfloat16)
    tokens, experts = token_ref.shape[0], NZ * group
    spots = experts * (FULL + TAIL)
    earlier_token = lax.broadcasted_iota(jnp.int32, (tokens, tokens), 1) < (
        lax.broadcasted_iota(jnp.int32, (tokens, tokens), 0)
    )
    earlier_token = jnp.where(earlier_token, 1.0, 0.0).astype(jnp.bfloat16)
    expert = lax.broadcasted_iota(jnp.int32, (tokens, experts), 1)
    spot = lax.broadcasted_iota(jnp.int32, (tokens, spots), 1)
    counted = jnp.zeros((1, experts), jnp.float32)
    chosen, combine = jnp.zeros((tokens, spots), jnp.float32), 0.0
    for route in range(2):
        named = ids_ref[:, route : route + 1]
        onehot = jnp.where(expert == named, 1.0, 0.0)
        rank = counted + jnp.dot(
            earlier_token, onehot.astype(jnp.bfloat16), preferred_element_type=jnp.float32
        )
        slot = jnp.sum(rank * onehot, axis=1, keepdims=True)
        counted = counted + jnp.sum(onehot, axis=0, keepdims=True)
        number = named.astype(jnp.float32)
        place = jnp.where(
            slot < FULL, number * FULL + slot, experts * FULL + number * TAIL + slot - FULL
        )
        hit = spot.astype(jnp.float32) == place
        chosen = jnp.where(hit, 1.0, chosen)
        combine = combine + jnp.where(hit, share_ref[:, route : route + 1], 0.0)
    combine_ref[...] = combine.astype(jnp.bfloat16)
    outgoing = lax.dot_general(
        chosen.astype(jnp.bfloat16), normed_own,
        (((0,), (0,)), ((), ())), preferred_element_type=jnp.float32,
    ).astype(jnp.bfloat16)
    main_ref[...] = outgoing[: experts * FULL].reshape(experts, FULL, COLS_T)
    tail_ref[...] = outgoing[experts * FULL :].reshape(experts, TAIL, COLS_T)
    pair_ref[0:BLOCK, :] = keys_ref[...]
    pair_ref[BLOCK:, :] = values_ref[...].T
    turned = queries_ref[...].T
    query_ref[0] = turned[:, :HALF]
    query_ref[1] = turned[:, HALF:]
    pl.semaphore_wait(barrier, NZ * NX * NC + 1)

    own_copies = [
        pltpu.make_async_copy(main_ref.at[me], xmain.at[me, :, own], own_sem.at[0]),
        pltpu.make_async_copy(tail_ref.at[me], xtail.at[me, :, own], own_sem.at[1]),
        pltpu.make_async_copy(pair_ref, pairs.at[z * NC + c], own_sem.at[2]),
        pltpu.make_async_copy(query_ref.at[0], parts.at[0, 0], own_sem.at[3]),
    ]
    for copy in own_copies:
        copy.start()

    for dz in (1, 7, 2, 6, 3, 5, 4, 0):
        to_z = lax.rem(z + dz, NZ)

        def send(step, carry):
            peer = lax.rem(local + step, group)
            device = (to_z, peer // NC, lax.rem(peer, NC), t)
            slab = to_z * group + peer
            for k, (source, target) in enumerate(((main_ref, xmain), (tail_ref, xtail))):
                remote(
                    source.at[slab], target.at[me, :, own],
                    out_send.at[k], out_recv.at[k, dz], device,
                ).start()
            return carry

        lax.fori_loop(1 if dz == 0 else 0, group, send, 0)

    mirrored = (NZ - 1 - z, x, c, t)
    remote(query_ref.at[1], parts.at[1, 0], q_send.at[3], q_recv.at[3], mirrored).start()
    for k in range(1, NX):
        device = (z, lax.rem(x + k, NX), c, t)
        remote(query_ref.at[0], parts.at[0, k], q_send.at[k - 1], q_recv.at[k - 1], device).start()

    higher, lower = (lax.rem(z + 1, NZ), x, c, t), (lax.rem(z + NZ - 1, NZ), x, c, t)
    across = (z, x, 1 - c, t)
    for way, device in enumerate((higher, lower)):
        remote(
            pair_ref, pairs.at[z * NC + c], kv_send.at[way, 0], kv_recv.at[way, 0], device
        ).start()
    remote(pair_ref, pairs.at[z * NC + c], c_send.at[0], c_recv.at[0], across).start()

    def rows_of(dz):
        return pl.ds(lax.rem(z - dz + NZ, NZ) * group, group)

    def y_copies(dz, slot, columns, device):
        rows = rows_of(dz)
        return [
            remote(
                target.at[rows, :, columns], target.at[rows, :, columns],
                y_send.at[slot, dz, k], y_recv.at[slot, dz, k], device,
            )
            for k, target in enumerate((xmain, xtail))
        ]

    to_after, to_before = (z, x, c, after), (z, x, c, before)

    def y_relay(dz):
        first = y_copies(dz, 0 if dz in PLUS else 1, own, to_after)
        for copy in first:
            copy.wait_recv()
        if dz in PLUS:
            copies = y_copies(dz, 2, columns_of(before), to_after)
        else:
            copies = y_copies(dz, 2, columns_of(after), to_before)
        for copy in copies:
            copy.start()

    def kv_step(step):
        for way, device in enumerate((higher, lower)):
            back = NZ - step if way == 0 else step
            block = lax.rem(z + back, NZ) * NC + c
            if step < 4:
                here = pairs.at[block]
                onward = here
                if step == 3:
                    onward = pairs.at[block, pl.ds(way * BLOCK, BLOCK), :]
            else:
                here = pairs.at[block, pl.ds(way * BLOCK, BLOCK), :]
            remote(
                here, here, kv_send.at[way, step - 1], kv_recv.at[way, step - 1], device
            ).wait_recv()
            if step < 4:
                remote(
                    onward, onward, kv_send.at[way, step], kv_recv.at[way, step], device
                ).start()
            slot = 2 * step - 1 + way
            remote(here, here, c_send.at[slot], c_recv.at[slot], across).start()

    opposite = lax.rem(t + 2, NT)
    devices = (to_after, to_before)
    far = NEAR[::-1]
    stages = (
        (fmain, relay_main, sum_main, in_main, red_main, rmain),
        (ftail, relay_tail, sum_tail, in_tail, red_tail, rtail),
    )

    def back_rows(dz):
        return pl.ds(lax.rem(z + dz, NZ) * group, group)

    def relay_copy(dz, k):
        source, target = stages[k][0], stages[k][1]
        return remote(
            source.at[back_rows(dz), :, columns_of(opposite)], target.at[dz],
            relay_send.at[dz, k], relay_recv.at[dz, k],
            to_after if dz in PLUS else to_before,
        )

    def s_copy(dz, k, way, source):
        return remote(
            source, stages[k][3].at[way, dz], s_send.at[way, dz, k], s_recv.at[way, dz, k],
            (to_after, to_before)[way],
        )

    def direct(dz, k):
        way = 1 if dz in PLUS else 0
        columns = columns_of((after, before)[way])
        return s_copy(dz, k, way, stages[k][0].at[back_rows(dz), :, columns])

    for copy in own_copies:
        copy.wait()
    for index, dz in enumerate(NEAR):
        count = group - 1 if dz == 0 else group
        first = 0 if dz == 0 else lax.rem(z - dz + NZ, NZ) * group
        rows = pl.ds(first, count)
        for k, (source, target) in enumerate(((main_ref, xmain), (tail_ref, xtail))):
            remote(
                source.at[pl.ds(0, count)], target.at[rows, :, own],
                out_send.at[k], out_recv.at[k, dz], higher,
            ).wait_recv()
        for slot, device in enumerate((to_after, to_before)):
            for copy in y_copies(dz, slot, own, device):
                copy.start()
        if index == 1:
            remote(
                query_ref.at[1], parts.at[1, 0], q_send.at[3], q_recv.at[3], mirrored
            ).wait_recv()
            for k in range(1, NX):
                device = (z, lax.rem(x + k, NX), c, t)
                remote(
                    parts.at[1, 0], parts.at[1, k], q_send.at[3 + k], q_recv.at[3 + k], device
                ).start()
        if index >= 2:
            y_relay(NEAR[index - 2])
    kv_step(1)
    y_relay(NEAR[6])
    y_relay(NEAR[7])
    kv_step(2)
    for dz in NEAR:
        for copy in y_copies(dz, 1 if dz in PLUS else 0, own, to_after):
            copy.wait_recv()
        for copy in y_copies(dz, 2, own, to_after):
            copy.wait_recv()
    for copy in weight_copies:
        copy.wait()
    slabs, width = NZ * group, hidden.shape[1]
    taken[0 : slabs * FULL] = xmain[...].reshape(slabs * FULL, NT * COLS_T)
    taken[slabs * FULL :] = xtail[...].reshape(slabs * TAIL, NT * COLS_T)
    for first in range(0, width, 256):
        cols = slice(first, min(first + 256, width))
        gate_act = jnp.dot(taken[...], gate[:, cols], preferred_element_type=jnp.float32)
        up_act = jnp.dot(taken[...], up[:, cols], preferred_element_type=jnp.float32)
        value = gate_act / (1.0 + jnp.exp(-gate_act)) * up_act
        hidden[:, cols] = value.astype(jnp.bfloat16)
    for turn in (2, 1, 3, 0):
        for part in range(2):
            start = lax.rem(t + turn, NT) * COLS_T + part * 256
            cols = pl.ds(pl.multiple_of(start, 256), 256)
            out = jnp.dot(hidden[...], down[:, cols], preferred_element_type=jnp.float32)
            out = out.astype(jnp.bfloat16)
            fmain[:, :, cols] = out[: slabs * FULL].reshape(slabs, FULL, 256)
            ftail[:, :, cols] = out[slabs * FULL :].reshape(slabs, TAIL, 256)
        for dz in far:
            for k in range(2):
                if turn == 2:
                    relay_copy(dz, k).start()
                elif turn == (3 if dz in PLUS else 1):
                    direct(dz, k).start()
    kv_step(3)
    def add_relay(dz):
        way = 0 if dz in PLUS else 1
        columns = columns_of((after, before)[way])
        for k in range(2):
            relay_copy(dz, k).wait_recv()
            source, relayed, total = stages[k][:3]
            mine = source[back_rows(dz), :, columns].astype(jnp.float32)
            total[dz] = (mine + relayed[dz].astype(jnp.float32)).astype(jnp.bfloat16)
            s_copy(dz, k, way, total.at[dz]).start()

    def finish(dz):
        to_z = lax.rem(z + dz, NZ)
        for k in range(2):
            source, arrived, reduced = stages[k][0], stages[k][3], stages[k][4]
            for way in range(2):
                s_copy(dz, k, way, stages[k][2].at[dz]).wait_recv()
            reduced[back_rows(dz)] = (
                source[back_rows(dz), :, columns_of(t)].astype(jnp.float32)
                + arrived[0, dz].astype(jnp.float32)
                + arrived[1, dz].astype(jnp.float32)
            ).astype(jnp.bfloat16)

        def send(step, carry):
            peer = lax.rem(local + step, group)
            device = (to_z, peer // NC, lax.rem(peer, NC), t)
            for k in range(2):
                remote(
                    stages[k][4].at[to_z * group + peer], stages[k][5].at[me],
                    back_send.at[k], back_recv.at[k], device,
                ).start()
            return carry

        lax.fori_loop(1 if dz == 0 else 0, group, send, 0)
        if dz == 0:
            for k in range(2):
                pltpu.make_async_copy(
                    stages[k][4].at[me], stages[k][5].at[me], r_sem.at[k]
                ).start()

    for slot in range(7):
        if slot != 3:
            remote(
                parts.at[0, 0], parts.at[0, 0], q_send.at[slot], q_recv.at[slot], higher
            ).wait_recv()
    map_row = lax.broadcasted_iota(jnp.int32, (128, HALF), 0)
    for way in range(2):
        for head in range(2):
            for step in range(NX):
                block = parts[way, step, head * 128 : (head + 1) * 128, :]
                for which in range(2):
                    first = (which * NX + step) * HALF
                    keep = (map_row < 64) if which == 0 else (map_row >= 64)
                    rhs_ref[head, way, :, first : first + HALF] = jnp.where(
                        keep, block, jnp.zeros_like(block)
                    )
    max_ref[...] = jnp.full_like(max_ref, LOW)
    acc_ref[...] = jnp.zeros_like(acc_ref)
    ones = jnp.ones((ACC - 128, CHUNK), jnp.bfloat16)
    tile = 256
    turns = 2 * NZ

    def work(head, way, step_z, masked):
        lanes = pl.ds(pl.multiple_of(head * 128, 128), 128)
        below = pl.ds(pl.multiple_of(256 + head * 128, 128), 128)
        keys = [pairs[step_z * NC + k, 0:256, lanes] for k in range(NC)]
        values = [pairs[step_z * NC + k, below, :] for k in range(NC)]
        keys = jnp.concatenate(keys, axis=0)
        values = jnp.concatenate([jnp.concatenate(values, axis=1), ones], axis=0)

        def score(slot, first):
            cols = slice(first, first + tile)
            scores = jnp.dot(keys, rhs_ref[head, way, :, cols], preferred_element_type=jnp.float32)
            if masked:
                key = lax.broadcasted_iota(jnp.int32, (CHUNK, tile), 0) + 2 * BLOCK * x
                col = lax.broadcasted_iota(jnp.int32, (1, tile), 1) + first
                query_x = lax.rem(x - (col // HALF) % NX + NX, NX)
                position = (2 * query_x + c) * BLOCK + way * HALF + col % HALF
                scores = jnp.where(position >= key, scores, -3e38)
            score_ref[slot] = scores

        score(0, 0)
        for number in range(COLS // tile):
            first = number * tile
            if first + tile < COLS:
                score((number + 1) % 2, first + tile)
            scores = score_ref[number % 2]
            cols = slice(first, first + tile)
            earlier = max_ref[way, 0:1, cols]
            now = jnp.maximum(earlier, jnp.max(scores, axis=0, keepdims=True))
            weights = jnp.exp2((scores - now) * EXP2_SCALE).astype(jnp.bfloat16)
            rescale = jnp.exp2((earlier - now) * EXP2_SCALE)
            max_ref[way, 0:1, cols] = now
            acc_ref[way, :, cols] = acc_ref[way, :, cols] * rescale + jnp.dot(
                values, weights, preferred_element_type=jnp.float32
            )

    def x_copy(head, k):
        maps = pl.ds(2 * head, 2)
        device = (z, lax.rem(x + NX - k, NX), c, t)
        return remote(
            partial.at[k, maps], others.at[k - 1, maps],
            p_send.at[head, k - 1], p_recv.at[head, k - 1], device,
        )

    def send_partial(head):
        row = lax.broadcasted_iota(jnp.int32, (ACC - 128, COLS), 0)
        for way in range(2):
            stats = jnp.zeros((ACC - 128, COLS), jnp.float32)
            pieces = pieces_of(acc_ref[way, 128:129, :]) + pieces_of(max_ref[way, 0:1, :])
            for index, piece in enumerate(pieces):
                stats = jnp.where(row == index, piece, stats)
            for which in range(2):
                for step in range(NX):
                    first = (which * NX + step) * HALF
                    lanes = slice(way * HALF, (way + 1) * HALF)
                    partial[step, 2 * head + which, 0:128, lanes] = acc_ref[
                        way, 0:128, first : first + HALF
                    ].astype(jnp.bfloat16)
                    partial[step, 2 * head + which, 128:ACC, lanes] = stats[
                        :, first : first + HALF
                    ].astype(jnp.bfloat16)
        for k in range(1, NX):
            x_copy(head, k).start()

    def peer_copy(slot):
        block = pairs.at[0] if slot < 7 else pairs.at[0, pl.ds(0, BLOCK), :]
        return remote(block, block, c_send.at[slot], c_recv.at[slot], across)

    def unit(index, carry):
        head = index // turns
        turn = lax.rem(index, turns)
        way = lax.rem(turn, 2)
        near = turn // 2
        distance = (near + 1) // 2
        step_z = lax.rem(z + jnp.where(lax.rem(near, 2) == 1, NZ - distance, distance), NZ)
        query_z = jnp.where(way == 0, z, NZ - 1 - z)
        for place, slots in ((0, (0,)), (2, (1,)), (4, (2,)), (6, (3,)), (8, (4,)), (10, (5,)), (12, (6,)), (14, (7, 8))):

            @pl.when(index == place)
            def _():
                for slot in slots:
                    peer_copy(slot).wait_recv()

        @pl.when(step_z == query_z)
        def _():
            work(head, way, step_z, True)

        @pl.when(step_z < query_z)
        def _():
            work(head, way, step_z, False)

        for k, dz in enumerate(far):

            @pl.when(index == 2 * k)
            def _():
                add_relay(dz)

            @pl.when(index == 2 * k + 3)
            def _():
                finish(dz)

        @pl.when(index == 7)
        def _():
            kv_step(4)

        @pl.when(index == turns - 1)
        def _():
            send_partial(0)
            max_ref[...] = jnp.full_like(max_ref, LOW)
            acc_ref[...] = jnp.zeros_like(acc_ref)

        return carry

    lax.fori_loop(0, 2 * turns, unit, 0)
    send_partial(1)

    gain_col = jnp.broadcast_to(gain_ref[...], (128, 128)).T[:, 0:1]
    for head in range(2):
        for k in range(1, NX):
            x_copy(head, k).wait_recv()
        per_map = []
        for which in range(2):
            index = 2 * head + which
            sources = [partial.at[0, index]] + [others.at[k, index] for k in range(NX - 1)]
            totals_of, maxima = [], []
            for part in sources:
                stats = part[128:ACC, :].astype(jnp.float32)
                totals_of.append(stats[0:1] + stats[1:2] + stats[2:3])
                maxima.append(stats[3:4] + stats[4:5] + stats[5:6])
            largest = functools.reduce(jnp.maximum, maxima)
            total, numerator = 0.0, 0.0
            for part, own_total, own_max in zip(sources, totals_of, maxima):
                factor = jnp.exp2((own_max - largest) * EXP2_SCALE)
                total = total + factor * own_total
                numerator = numerator + factor * part[0:128, :].astype(jnp.float32)
            per_map.append(numerator / total)
        contrast = per_map[0] - lambda_ref[head] * per_map[1]
        square = jnp.mean(contrast * contrast, axis=0, keepdims=True)
        normed = contrast * lax.rsqrt(square + EPS) * gain_col
        normed = normed.astype(jnp.bfloat16)
        attended[head * 128 : (head + 1) * 128, :] = normed[:, :HALF]
        upper_send[head * 128 : (head + 1) * 128, :] = normed[:, HALF:]

    flip = remote(upper_send, upper_recv, u_send, u_recv, mirrored)
    flip.start()
    rows = BLOCK // NT
    half = rows // 2

    def project(source, first):
        for low in range(0, 2048, 512):
            part = lax.dot_general(
                source[...], weight_ref[:, low : low + 512],
                (((0,), (0,)), ((), ())), preferred_element_type=jnp.float32,
            ).astype(jnp.bfloat16)
            blocks[first, :, low : low + 512] = part[:rows]
            blocks[first + 1, :, low : low + 512] = part[rows:]

    project(attended, 0)
    flip.wait()
    project(upper_recv, 2)

    def mix_relay(way):
        return remote(
            blocks.at[opposite, pl.ds(way * half, half), :], relayed.at[way],
            mix_send.at[way], mix_recv.at[way], devices[way],
        )

    def mix_copy(way, part, source):
        return remote(
            source, arrived_y.at[way, pl.ds(part * half, half), :],
            sum_send.at[way, part], sum_recv.at[way, part], devices[way],
        )

    for way in range(2):
        mix_relay(way).start()
    for way in range(2):
        source = blocks.at[(after, before)[way], pl.ds((1 - way) * half, half), :]
        mix_copy(way, 1 - way, source).start()
    for way in range(2):
        mix_relay(way).wait_recv()
        mine = blocks[(after, before)[way], way * half : (way + 1) * half, :]
        totals[way] = (
            mine.astype(jnp.float32) + relayed[way].astype(jnp.float32)
        ).astype(jnp.bfloat16)
        mix_copy(way, way, totals.at[way]).start()
    for k in range(2):
        pltpu.make_async_copy(stages[k][4].at[me], stages[k][5].at[me], r_sem.at[k]).wait()
        every = pl.ds(0, NZ * group - 1)
        copy = remote(
            stages[k][4].at[every], stages[k][5].at[every], back_send.at[k], back_recv.at[k], to_after
        )
        copy.wait_recv()
        copy.wait_send()
        for dz in far:
            relay_copy(dz, k).wait_send()
            for way in range(2):
                s_copy(dz, k, way, stages[k][2].at[dz]).wait_send()
    full = experts * FULL
    mixed_ref[...] = (
        jnp.dot(
            combine_ref[:, :full], rmain[...].reshape(full, COLS_T),
            preferred_element_type=jnp.float32,
        )
        + jnp.dot(
            combine_ref[:, full:], rtail[...].reshape(spots - full, COLS_T),
            preferred_element_type=jnp.float32,
        )
    ).astype(jnp.bfloat16)
    for way in range(2):
        for part in range(2):
            copy = mix_copy(way, part, totals.at[way])
            copy.wait_recv()
            copy.wait_send()
        mix_relay(way).wait_send()
    out_ref[...] = (
        blocks[t].astype(jnp.float32)
        + arrived_y[0].astype(jnp.float32)
        + arrived_y[1].astype(jnp.float32)
    ).astype(jnp.bfloat16)

    for head in range(2):
        for k in range(1, NX):
            x_copy(head, k).wait_send()

    for dz in NEAR:
        for slot in range(3):
            for copy in y_copies(dz, slot, own, to_after):
                copy.wait_send()
    for k, (source, target) in enumerate(((main_ref, xmain), (tail_ref, xtail))):
        every = pl.ds(0, NZ * group - 1)
        remote(
            source.at[every], target.at[every, :, own], out_send.at[k], out_recv.at[k, 0], higher
        ).wait_send()
    for way in range(2):
        for step in range(4):
            block = pairs.at[0] if step < 3 else pairs.at[0, pl.ds(0, BLOCK), :]
            remote(block, block, kv_send.at[way, step], kv_recv.at[way, step], higher).wait_send()
    for slot in range(9):
        block = pairs.at[0] if slot < 7 else pairs.at[0, pl.ds(0, BLOCK), :]
        remote(block, block, c_send.at[slot], c_recv.at[slot], across).wait_send()
    for slot in range(7):
        remote(
            parts.at[0, 0], parts.at[0, 0], q_send.at[slot], q_recv.at[slot], higher
        ).wait_send()


VMEM = pl.BlockSpec(memory_space=pltpu.VMEM)
HBM = pl.BlockSpec(memory_space=pl.ANY)


def layer_call(
    queries, key_rows, value_rows, head_lambda, sub_gain, out_weight, expert_input, norm_gain,
    route_ids, route_weight, gate, up, down,
):
    dma = pltpu.SemaphoreType.DMA
    slabs, group = NZ * NX * NC, NX * NC
    units = gate.shape[1]
    rows, width = BLOCK // NT, out_weight.shape[1]
    tokens = expert_input.shape[0]
    bf16, f32 = jnp.bfloat16, jnp.float32

    def both(*lead, columns=COLS_T):
        return [pltpu.VMEM((*lead, count, columns), bf16) for count in (FULL, TAIL)]

    return pl.pallas_call(
        layer_kernel,
        out_shape=(
            jax.ShapeDtypeStruct((rows, width), bf16),
            jax.ShapeDtypeStruct((tokens, COLS_T), bf16),
        ),
        in_specs=[pl.BlockSpec(memory_space=pltpu.SMEM)] + [VMEM] * 9 + [HBM] * 3,
        out_specs=(VMEM,) * 2,
        scratch_shapes=[
            *both(slabs),
            pltpu.VMEM((2 * BLOCK, BLOCK), bf16),
            pltpu.VMEM((2, BLOCK, HALF), bf16),
            pltpu.VMEM((tokens, slabs * (FULL + TAIL)), bf16),
            *both(slabs),
            *both(slabs, columns=width),
            pltpu.VMEM((slabs * (FULL + TAIL), width), bf16),
            pltpu.VMEM((slabs * (FULL + TAIL), units), bf16),
            pltpu.VMEM((width, units), bf16),
            pltpu.VMEM((width, units), bf16),
            pltpu.VMEM((units, width), bf16),
            *both(slabs, columns=width),
            pltpu.VMEM((NZ * NC, 2 * BLOCK, BLOCK), bf16),
            pltpu.VMEM((2, NX, BLOCK, HALF), bf16),
            pltpu.VMEM((2, 2, 128, COLS), bf16),
            pltpu.VMEM((2, CHUNK, 256), f32),
            pltpu.VMEM((2, 8, COLS), f32),
            pltpu.VMEM((2, ACC, COLS), f32),
            pltpu.VMEM((NX, 4, ACC, BLOCK), bf16),
            pltpu.VMEM((NX - 1, 4, ACC, BLOCK), bf16),
            pltpu.VMEM((BLOCK, HALF), bf16),
            pltpu.VMEM((BLOCK, HALF), bf16),
            pltpu.VMEM((BLOCK, HALF), bf16),
            pltpu.VMEM((NT, rows, width), bf16),
            pltpu.VMEM((2, rows // 2, width), bf16),
            pltpu.VMEM((2, rows // 2, width), bf16),
            pltpu.VMEM((2, rows, width), bf16),
            *both(NZ, group), *both(NZ, group), *both(2, NZ, group), *both(slabs),
            dma((3,)), dma((4,)), dma((2,)), dma((2, NZ)), dma((3, NZ, 2)), dma((3, NZ, 2)),
            dma((2, 4)), dma((2, 4)), dma((9,)), dma((9,)), dma((7,)), dma((7,)),
            dma((2,)), dma((2, 3)), dma((2, 3)), dma((NZ, 2)), dma((NZ, 2)),
            dma((2, NZ, 2)), dma((2, NZ, 2)), dma((2,)), dma((2,)),
            dma(()), dma(()), dma((2,)), dma((2,)), dma((2, 2)), dma((2, 2)),
        ],
        compiler_params=pltpu.CompilerParams(
            collective_id=0, has_side_effects=True, vmem_limit_bytes=56 * 2**20
        ),
        name="layer",
    )(
        head_lambda, sub_gain[None, :], key_rows, value_rows, queries, expert_input,
        norm_gain[None, :], route_ids, route_weight, out_weight, gate, up, down,
    )


def shards(
    queries,
    key_rows,
    value_rows,
    head_lambda,
    sub_gain,
    out_weight,
    expert_input,
    norm_gain,
    route_ids,
    route_weight,
    gate_weight,
    up_weight,
    down_weight,
):
    return layer_call(
        queries, key_rows, value_rows, head_lambda, sub_gain, out_weight, expert_input, norm_gain,
        route_ids, route_weight, gate_weight[0], up_weight[0], down_weight[0],
    )


def solution(mesh):
    mesh = Mesh(mesh.devices.reshape(NZ, NX, NC, NT), (*EP, "tp"))
    placed = (
        P(EP, "tp"),
        P(EP, "tp"),
        P(EP, "tp"),
        P("tp"),
        P(),
        P("tp", None),
        P(EP, None),
        P(),
        P(EP, None),
        P(EP, None),
        P(EP, None, "tp"),
        P(EP, None, "tp"),
        P(EP, "tp", None),
    )
    return jax.shard_map(
        shards,
        mesh=mesh,
        in_specs=placed,
        out_specs=(P((*EP, "tp"), None), P(EP, "tp")),
        check_vma=False,
    )
```

```python
import functools
import math

import jax
import jax.numpy as jnp
from jax import lax
from jax.experimental import pallas as pl
from jax.experimental.pallas import tpu as pltpu
from jax.sharding import Mesh, PartitionSpec as P

EPS = 1e-06
NZ, NX, NC, NT = 8, 4, 2, 4
EP = ("z", "x", "core")
BLOCK = 256
HALF = BLOCK // 2
CHUNK = NC * BLOCK
COLS = 2 * NX * HALF
ACC = 144
COLS_T = 512
FULL, TAIL = 8, 2
NEAR = (0, 1, 7, 2, 6, 3, 5, 4)
PLUS = (0, 7, 6, 5)
LOW = -1e30
EXP2_SCALE = 64 ** (-0.5) * math.log2(math.e)


def pieces_of(value):
    first = value.astype(jnp.bfloat16).astype(jnp.float32)
    second = (value - first).astype(jnp.bfloat16).astype(jnp.float32)
    third = value - first - second
    return first, second, third


def places():
    return tuple(lax.axis_index(name) for name in (*EP, "tp"))


def remote(source, target, send, receive, device):
    return pltpu.make_async_remote_copy(
        src_ref=source,
        dst_ref=target,
        send_sem=send,
        recv_sem=receive,
        device_id=device,
        device_id_type=pl.DeviceIdType.MESH,
    )


def greet_all(z, x, c, t):
    me = (z * NX + x) * NC + c
    barrier = pltpu.get_barrier_semaphore()

    def signal(step, carry):
        peer = lax.rem(me + step, NZ * NX * NC)
        device = (peer // (NX * NC), lax.rem(peer // NC, NX), lax.rem(peer, NC), t)
        pl.semaphore_signal(
            barrier, inc=1, device_id=device, device_id_type=pl.DeviceIdType.MESH
        )
        return carry

    for dy in (1, NT - 1):
        pl.semaphore_signal(
            barrier,
            inc=1,
            device_id=(z, x, c, lax.rem(t + dy, NT)),
            device_id_type=pl.DeviceIdType.MESH,
        )
    lax.fori_loop(1, NZ * NX * NC, signal, 0)
    return barrier


def columns_of(t):
    return pl.ds(pl.multiple_of(t * COLS_T, COLS_T), COLS_T)


def layer_kernel(
    lambda_ref, gain_ref, keys_ref, values_ref, queries_ref, token_ref, norm_ref, ids_ref,
    share_ref, weight_ref, gate_ref, up_ref, down_ref,
    out_ref, mixed_ref,
    main_ref, tail_ref, pair_ref, query_ref, combine_ref, rmain, rtail,
    xmain, xtail, taken, hidden, gate, up, down, fmain, ftail, pairs, parts,
    rhs_ref, score_ref, max_ref, acc_ref, partial, others,
    attended, upper_send, upper_recv, blocks, relayed, totals, arrived_y,
    relay_main, relay_tail, sum_main, sum_tail, in_main, in_tail, red_main, red_tail,
    w_sem, own_sem, out_send, out_recv, y_send, y_recv, kv_send, kv_recv, c_send, c_recv,
    q_send, q_recv, r_sem, p_send, p_recv, relay_send, relay_recv, s_send, s_recv,
    back_send, back_recv, u_send, u_recv, mix_send, mix_recv, sum_send, sum_recv,
):
    z, x, c, t = places()
    me = (z * NX + x) * NC + c
    local = x * NC + c
    group = NX * NC
    after, before = lax.rem(t + 1, NT), lax.rem(t + NT - 1, NT)
    own = columns_of(t)
    weight_copies = [
        pltpu.make_async_copy(source, target, w_sem.at[k])
        for k, (source, target) in enumerate(((gate_ref, gate), (up_ref, up), (down_ref, down)))
    ]
    for copy in weight_copies:
        copy.start()
    barrier = greet_all(z, x, c, t)

    wide = token_ref[...].astype(jnp.float32)
    scale = lax.rsqrt(jnp.mean(wide * wide, axis=-1, keepdims=True) + EPS)
    normed_own = token_ref[:, own].astype(jnp.float32) * scale * norm_ref[:, own]
    normed_own = normed_own.astype(jnp.bfloat16)
    tokens, experts = token_ref.shape[0], NZ * group
    spots = experts * (FULL + TAIL)
    earlier_token = lax.broadcasted_iota(jnp.int32, (tokens, tokens), 1) < (
        lax.broadcasted_iota(jnp.int32, (tokens, tokens), 0)
    )
    earlier_token = jnp.where(earlier_token, 1.0, 0.0).astype(jnp.bfloat16)
    expert = lax.broadcasted_iota(jnp.int32, (tokens, experts), 1)
    spot = lax.broadcasted_iota(jnp.int32, (tokens, spots), 1)
    counted = jnp.zeros((1, experts), jnp.float32)
    chosen, combine = jnp.zeros((tokens, spots), jnp.float32), 0.0
    names, shares = ids_ref[...].T, share_ref[...].T
    for route in range(2):
        named = names[:, route : route + 1]
        onehot = jnp.where(expert == named, 1.0, 0.0)
        rank = counted + jnp.dot(
            earlier_token, onehot.astype(jnp.bfloat16), preferred_element_type=jnp.float32
        )
        slot = jnp.sum(rank * onehot, axis=1, keepdims=True)
        counted = counted + jnp.sum(onehot, axis=0, keepdims=True)
        number = named.astype(jnp.float32)
        place = jnp.where(
            slot < FULL, number * FULL + slot, experts * FULL + number * TAIL + slot - FULL
        )
        hit = spot.astype(jnp.float32) == place
        chosen = jnp.where(hit, 1.0, chosen)
        combine = combine + jnp.where(hit, shares[:, route : route + 1], 0.0)
    combine_ref[...] = combine.astype(jnp.bfloat16)
    outgoing = lax.dot_general(
        chosen.astype(jnp.bfloat16), normed_own,
        (((0,), (0,)), ((), ())), preferred_element_type=jnp.float32,
    ).astype(jnp.bfloat16)
    main_ref[...] = outgoing[: experts * FULL].reshape(experts, FULL, COLS_T)
    tail_ref[...] = outgoing[experts * FULL :].reshape(experts, TAIL, COLS_T)
    pair_ref[0:BLOCK, :] = keys_ref[...]
    pair_ref[BLOCK:, :] = values_ref[...].T
    turned = queries_ref[...].T
    query_ref[0] = turned[:, :HALF]
    query_ref[1] = turned[:, HALF:]
    pl.semaphore_wait(barrier, NZ * NX * NC + 1)

    own_copies = [
        pltpu.make_async_copy(main_ref.at[me], xmain.at[me, :, own], own_sem.at[0]),
        pltpu.make_async_copy(tail_ref.at[me], xtail.at[me, :, own], own_sem.at[1]),
        pltpu.make_async_copy(pair_ref, pairs.at[z * NC + c], own_sem.at[2]),
        pltpu.make_async_copy(query_ref.at[0], parts.at[0, 0], own_sem.at[3]),
    ]
    for copy in own_copies:
        copy.start()

    for dz in (1, 7, 2, 6, 3, 5, 4, 0):
        to_z = lax.rem(z + dz, NZ)

        def send(step, carry):
            peer = lax.rem(local + step, group)
            device = (to_z, peer // NC, lax.rem(peer, NC), t)
            slab = to_z * group + peer
            for k, (source, target) in enumerate(((main_ref, xmain), (tail_ref, xtail))):
                remote(
                    source.at[slab], target.at[me, :, own],
                    out_send.at[k], out_recv.at[k, dz], device,
                ).start()
            return carry

        lax.fori_loop(1 if dz == 0 else 0, group, send, 0)

    mirrored = (NZ - 1 - z, x, c, t)
    remote(query_ref.at[1], parts.at[1, 0], q_send.at[3], q_recv.at[3], mirrored).start()
    for k in range(1, NX):
        device = (z, lax.rem(x + k, NX), c, t)
        remote(query_ref.at[0], parts.at[0, k], q_send.at[k - 1], q_recv.at[k - 1], device).start()

    higher, lower = (lax.rem(z + 1, NZ), x, c, t), (lax.rem(z + NZ - 1, NZ), x, c, t)
    across = (z, x, 1 - c, t)
    for way, device in enumerate((higher, lower)):
        remote(
            pair_ref, pairs.at[z * NC + c], kv_send.at[way, 0], kv_recv.at[way, 0], device
        ).start()
    remote(pair_ref, pairs.at[z * NC + c], c_send.at[0], c_recv.at[0], across).start()

    def rows_of(dz):
        return pl.ds(lax.rem(z - dz + NZ, NZ) * group, group)

    def y_copies(dz, slot, columns, device):
        rows = rows_of(dz)
        return [
            remote(
                target.at[rows, :, columns], target.at[rows, :, columns],
                y_send.at[slot, dz, k], y_recv.at[slot, dz, k], device,
            )
            for k, target in enumerate((xmain, xtail))
        ]

    to_after, to_before = (z, x, c, after), (z, x, c, before)

    def y_relay(dz):
        first = y_copies(dz, 0 if dz in PLUS else 1, own, to_after)
        for copy in first:
            copy.wait_recv()
        if dz in PLUS:
            copies = y_copies(dz, 2, columns_of(before), to_after)
        else:
            copies = y_copies(dz, 2, columns_of(after), to_before)
        for copy in copies:
            copy.start()

    def kv_step(step):
        for way, device in enumerate((higher, lower)):
            back = NZ - step if way == 0 else step
            block = lax.rem(z + back, NZ) * NC + c
            if step < 4:
                here = pairs.at[block]
                onward = here
                if step == 3:
                    onward = pairs.at[block, pl.ds(way * BLOCK, BLOCK), :]
            else:
                here = pairs.at[block, pl.ds(way * BLOCK, BLOCK), :]
            remote(
                here, here, kv_send.at[way, step - 1], kv_recv.at[way, step - 1], device
            ).wait_recv()
            if step < 4:
                remote(
                    onward, onward, kv_send.at[way, step], kv_recv.at[way, step], device
                ).start()
            slot = 2 * step - 1 + way
            remote(here, here, c_send.at[slot], c_recv.at[slot], across).start()

    opposite = lax.rem(t + 2, NT)
    devices = (to_after, to_before)
    far = NEAR[::-1]
    stages = (
        (fmain, relay_main, sum_main, in_main, red_main, rmain),
        (ftail, relay_tail, sum_tail, in_tail, red_tail, rtail),
    )

    def back_rows(dz):
        return pl.ds(lax.rem(z + dz, NZ) * group, group)

    def relay_copy(dz, k):
        source, target = stages[k][0], stages[k][1]
        return remote(
            source.at[back_rows(dz), :, columns_of(opposite)], target.at[dz],
            relay_send.at[dz, k], relay_recv.at[dz, k],
            to_after if dz in PLUS else to_before,
        )

    def s_copy(dz, k, way, source):
        return remote(
            source, stages[k][3].at[way, dz], s_send.at[way, dz, k], s_recv.at[way, dz, k],
            (to_after, to_before)[way],
        )

    def direct(dz, k):
        way = 1 if dz in PLUS else 0
        columns = columns_of((after, before)[way])
        return s_copy(dz, k, way, stages[k][0].at[back_rows(dz), :, columns])

    for copy in own_copies:
        copy.wait()
    for index, dz in enumerate(NEAR):
        count = group - 1 if dz == 0 else group
        first = 0 if dz == 0 else lax.rem(z - dz + NZ, NZ) * group
        rows = pl.ds(first, count)
        for k, (source, target) in enumerate(((main_ref, xmain), (tail_ref, xtail))):
            remote(
                source.at[pl.ds(0, count)], target.at[rows, :, own],
                out_send.at[k], out_recv.at[k, dz], higher,
            ).wait_recv()
        for slot, device in enumerate((to_after, to_before)):
            for copy in y_copies(dz, slot, own, device):
                copy.start()
        if index == 1:
            remote(
                query_ref.at[1], parts.at[1, 0], q_send.at[3], q_recv.at[3], mirrored
            ).wait_recv()
            for k in range(1, NX):
                device = (z, lax.rem(x + k, NX), c, t)
                remote(
                    parts.at[1, 0], parts.at[1, k], q_send.at[3 + k], q_recv.at[3 + k], device
                ).start()
        if index >= 2:
            y_relay(NEAR[index - 2])
    kv_step(1)
    y_relay(NEAR[6])
    y_relay(NEAR[7])
    kv_step(2)
    for dz in NEAR:
        for copy in y_copies(dz, 1 if dz in PLUS else 0, own, to_after):
            copy.wait_recv()
        for copy in y_copies(dz, 2, own, to_after):
            copy.wait_recv()
    for copy in weight_copies:
        copy.wait()
    slabs, width = NZ * group, hidden.shape[1]
    taken[0 : slabs * FULL] = xmain[...].reshape(slabs * FULL, NT * COLS_T)
    taken[slabs * FULL :] = xtail[...].reshape(slabs * TAIL, NT * COLS_T)
    for first in range(0, width, 256):
        cols = slice(first, min(first + 256, width))
        gate_act = jnp.dot(taken[...], gate[:, cols], preferred_element_type=jnp.float32)
        up_act = jnp.dot(taken[...], up[:, cols], preferred_element_type=jnp.float32)
        value = gate_act / (1.0 + jnp.exp(-gate_act)) * up_act
        hidden[:, cols] = value.astype(jnp.bfloat16)
    for turn in (2, 1, 3, 0):
        for part in range(2):
            start = lax.rem(t + turn, NT) * COLS_T + part * 256
            cols = pl.ds(pl.multiple_of(start, 256), 256)
            out = jnp.dot(hidden[...], down[:, cols], preferred_element_type=jnp.float32)
            out = out.astype(jnp.bfloat16)
            fmain[:, :, cols] = out[: slabs * FULL].reshape(slabs, FULL, 256)
            ftail[:, :, cols] = out[slabs * FULL :].reshape(slabs, TAIL, 256)
        for dz in far:
            for k in range(2):
                if turn == 2:
                    relay_copy(dz, k).start()
                elif turn == (3 if dz in PLUS else 1):
                    direct(dz, k).start()
    kv_step(3)
    def add_relay(dz):
        way = 0 if dz in PLUS else 1
        columns = columns_of((after, before)[way])
        for k in range(2):
            relay_copy(dz, k).wait_recv()
            source, relayed, total = stages[k][:3]
            mine = source[back_rows(dz), :, columns].astype(jnp.float32)
            total[dz] = (mine + relayed[dz].astype(jnp.float32)).astype(jnp.bfloat16)
            s_copy(dz, k, way, total.at[dz]).start()

    def finish(dz):
        to_z = lax.rem(z + dz, NZ)
        for k in range(2):
            source, arrived, reduced = stages[k][0], stages[k][3], stages[k][4]
            for way in range(2):
                s_copy(dz, k, way, stages[k][2].at[dz]).wait_recv()
            reduced[back_rows(dz)] = (
                source[back_rows(dz), :, columns_of(t)].astype(jnp.float32)
                + arrived[0, dz].astype(jnp.float32)
                + arrived[1, dz].astype(jnp.float32)
            ).astype(jnp.bfloat16)

        def send(step, carry):
            peer = lax.rem(local + step, group)
            device = (to_z, peer // NC, lax.rem(peer, NC), t)
            for k in range(2):
                remote(
                    stages[k][4].at[to_z * group + peer], stages[k][5].at[me],
                    back_send.at[k], back_recv.at[k], device,
                ).start()
            return carry

        lax.fori_loop(1 if dz == 0 else 0, group, send, 0)
        if dz == 0:
            for k in range(2):
                pltpu.make_async_copy(
                    stages[k][4].at[me], stages[k][5].at[me], r_sem.at[k]
                ).start()

    for slot in range(7):
        if slot != 3:
            remote(
                parts.at[0, 0], parts.at[0, 0], q_send.at[slot], q_recv.at[slot], higher
            ).wait_recv()
    map_row = lax.broadcasted_iota(jnp.int32, (128, HALF), 0)
    for way in range(2):
        for head in range(2):
            for step in range(NX):
                block = parts[way, step, head * 128 : (head + 1) * 128, :]
                for which in range(2):
                    first = (which * NX + step) * HALF
                    keep = (map_row < 64) if which == 0 else (map_row >= 64)
                    rhs_ref[head, way, :, first : first + HALF] = jnp.where(
                        keep, block, jnp.zeros_like(block)
                    )
    max_ref[...] = jnp.full_like(max_ref, LOW)
    acc_ref[...] = jnp.zeros_like(acc_ref)
    ones = jnp.ones((ACC - 128, CHUNK), jnp.bfloat16)
    tile = 256
    turns = 2 * NZ

    def work(head, way, step_z, masked):
        lanes = pl.ds(pl.multiple_of(head * 128, 128), 128)
        below = pl.ds(pl.multiple_of(256 + head * 128, 128), 128)
        keys = [pairs[step_z * NC + k, 0:256, lanes] for k in range(NC)]
        values = [pairs[step_z * NC + k, below, :] for k in range(NC)]
        keys = jnp.concatenate(keys, axis=0)
        values = jnp.concatenate([jnp.concatenate(values, axis=1), ones], axis=0)

        def score(slot, first):
            cols = slice(first, first + tile)
            scores = jnp.dot(keys, rhs_ref[head, way, :, cols], preferred_element_type=jnp.float32)
            if masked:
                key = lax.broadcasted_iota(jnp.int32, (CHUNK, tile), 0) + 2 * BLOCK * x
                col = lax.broadcasted_iota(jnp.int32, (1, tile), 1) + first
                query_x = lax.rem(x - (col // HALF) % NX + NX, NX)
                position = (2 * query_x + c) * BLOCK + way * HALF + col % HALF
                scores = jnp.where(position >= key, scores, -3e38)
            score_ref[slot] = scores

        score(0, 0)
        for number in range(COLS // tile):
            first = number * tile
            if first + tile < COLS:
                score((number + 1) % 2, first + tile)
            scores = score_ref[number % 2]
            cols = slice(first, first + tile)
            earlier = max_ref[way, 0:1, cols]
            now = jnp.maximum(earlier, jnp.max(scores, axis=0, keepdims=True))
            weights = jnp.exp2((scores - now) * EXP2_SCALE).astype(jnp.bfloat16)
            rescale = jnp.exp2((earlier - now) * EXP2_SCALE)
            max_ref[way, 0:1, cols] = now
            acc_ref[way, :, cols] = acc_ref[way, :, cols] * rescale + jnp.dot(
                values, weights, preferred_element_type=jnp.float32
            )

    def x_copy(head, k):
        maps = pl.ds(2 * head, 2)
        device = (z, lax.rem(x + NX - k, NX), c, t)
        return remote(
            partial.at[k, maps], others.at[k - 1, maps],
            p_send.at[head, k - 1], p_recv.at[head, k - 1], device,
        )

    def send_partial(head):
        row = lax.broadcasted_iota(jnp.int32, (ACC - 128, COLS), 0)
        for way in range(2):
            stats = jnp.zeros((ACC - 128, COLS), jnp.float32)
            pieces = pieces_of(acc_ref[way, 128:129, :]) + pieces_of(max_ref[way, 0:1, :])
            for index, piece in enumerate(pieces):
                stats = jnp.where(row == index, piece, stats)
            for which in range(2):
                for step in range(NX):
                    first = (which * NX + step) * HALF
                    lanes = slice(way * HALF, (way + 1) * HALF)
                    partial[step, 2 * head + which, 0:128, lanes] = acc_ref[
                        way, 0:128, first : first + HALF
                    ].astype(jnp.bfloat16)
                    partial[step, 2 * head + which, 128:ACC, lanes] = stats[
                        :, first : first + HALF
                    ].astype(jnp.bfloat16)
        for k in range(1, NX):
            x_copy(head, k).start()

    def peer_copy(slot):
        block = pairs.at[0] if slot < 7 else pairs.at[0, pl.ds(0, BLOCK), :]
        return remote(block, block, c_send.at[slot], c_recv.at[slot], across)

    def unit(index, carry):
        head = index // turns
        turn = lax.rem(index, turns)
        way = lax.rem(turn, 2)
        near = turn // 2
        distance = (near + 1) // 2
        step_z = lax.rem(z + jnp.where(lax.rem(near, 2) == 1, NZ - distance, distance), NZ)
        query_z = jnp.where(way == 0, z, NZ - 1 - z)
        for place, slots in ((0, (0,)), (2, (1,)), (4, (2,)), (6, (3,)), (8, (4,)), (10, (5,)), (12, (6,)), (14, (7, 8))):

            @pl.when(index == place)
            def _():
                for slot in slots:
                    peer_copy(slot).wait_recv()

        @pl.when(step_z == query_z)
        def _():
            work(head, way, step_z, True)

        @pl.when(step_z < query_z)
        def _():
            work(head, way, step_z, False)

        for k, dz in enumerate(far):

            @pl.when(index == 2 * k)
            def _():
                add_relay(dz)

            @pl.when(index == 2 * k + 3)
            def _():
                finish(dz)

        @pl.when(index == 7)
        def _():
            kv_step(4)

        @pl.when(index == turns - 1)
        def _():
            send_partial(0)
            max_ref[...] = jnp.full_like(max_ref, LOW)
            acc_ref[...] = jnp.zeros_like(acc_ref)

        return carry

    lax.fori_loop(0, 2 * turns, unit, 0)
    send_partial(1)

    gain_col = jnp.broadcast_to(gain_ref[...], (128, 128)).T[:, 0:1]
    for head in range(2):
        for k in range(1, NX):
            x_copy(head, k).wait_recv()
        per_map = []
        for which in range(2):
            index = 2 * head + which
            sources = [partial.at[0, index]] + [others.at[k, index] for k in range(NX - 1)]
            totals_of, maxima = [], []
            for part in sources:
                stats = part[128:ACC, :].astype(jnp.float32)
                totals_of.append(stats[0:1] + stats[1:2] + stats[2:3])
                maxima.append(stats[3:4] + stats[4:5] + stats[5:6])
            largest = functools.reduce(jnp.maximum, maxima)
            total, numerator = 0.0, 0.0
            for part, own_total, own_max in zip(sources, totals_of, maxima):
                factor = jnp.exp2((own_max - largest) * EXP2_SCALE)
                total = total + factor * own_total
                numerator = numerator + factor * part[0:128, :].astype(jnp.float32)
            per_map.append(numerator / total)
        contrast = per_map[0] - lambda_ref[head] * per_map[1]
        square = jnp.mean(contrast * contrast, axis=0, keepdims=True)
        normed = contrast * lax.rsqrt(square + EPS) * gain_col
        normed = normed.astype(jnp.bfloat16)
        attended[head * 128 : (head + 1) * 128, :] = normed[:, :HALF]
        upper_send[head * 128 : (head + 1) * 128, :] = normed[:, HALF:]

    flip = remote(upper_send, upper_recv, u_send, u_recv, mirrored)
    flip.start()
    rows = BLOCK // NT
    half = rows // 2

    def project(source, first):
        for low in range(0, 2048, 512):
            part = lax.dot_general(
                source[...], weight_ref[:, low : low + 512],
                (((0,), (0,)), ((), ())), preferred_element_type=jnp.float32,
            ).astype(jnp.bfloat16)
            blocks[first, :, low : low + 512] = part[:rows]
            blocks[first + 1, :, low : low + 512] = part[rows:]

    project(attended, 0)
    flip.wait()
    project(upper_recv, 2)

    def mix_relay(way):
        return remote(
            blocks.at[opposite, pl.ds(way * half, half), :], relayed.at[way],
            mix_send.at[way], mix_recv.at[way], devices[way],
        )

    def mix_copy(way, part, source):
        return remote(
            source, arrived_y.at[way, pl.ds(part * half, half), :],
            sum_send.at[way, part], sum_recv.at[way, part], devices[way],
        )

    for way in range(2):
        mix_relay(way).start()
    for way in range(2):
        source = blocks.at[(after, before)[way], pl.ds((1 - way) * half, half), :]
        mix_copy(way, 1 - way, source).start()
    for way in range(2):
        mix_relay(way).wait_recv()
        mine = blocks[(after, before)[way], way * half : (way + 1) * half, :]
        totals[way] = (
            mine.astype(jnp.float32) + relayed[way].astype(jnp.float32)
        ).astype(jnp.bfloat16)
        mix_copy(way, way, totals.at[way]).start()
    for k in range(2):
        pltpu.make_async_copy(stages[k][4].at[me], stages[k][5].at[me], r_sem.at[k]).wait()
        every = pl.ds(0, NZ * group - 1)
        copy = remote(
            stages[k][4].at[every], stages[k][5].at[every], back_send.at[k], back_recv.at[k], to_after
        )
        copy.wait_recv()
        copy.wait_send()
        for dz in far:
            relay_copy(dz, k).wait_send()
            for way in range(2):
                s_copy(dz, k, way, stages[k][2].at[dz]).wait_send()
    full = experts * FULL
    mixed_ref[...] = (
        jnp.dot(
            combine_ref[:, :full], rmain[...].reshape(full, COLS_T),
            preferred_element_type=jnp.float32,
        )
        + jnp.dot(
            combine_ref[:, full:], rtail[...].reshape(spots - full, COLS_T),
            preferred_element_type=jnp.float32,
        )
    ).astype(jnp.bfloat16)
    for way in range(2):
        for part in range(2):
            copy = mix_copy(way, part, totals.at[way])
            copy.wait_recv()
            copy.wait_send()
        mix_relay(way).wait_send()
    out_ref[...] = (
        blocks[t].astype(jnp.float32)
        + arrived_y[0].astype(jnp.float32)
        + arrived_y[1].astype(jnp.float32)
    ).astype(jnp.bfloat16)

    for head in range(2):
        for k in range(1, NX):
            x_copy(head, k).wait_send()

    for dz in NEAR:
        for slot in range(3):
            for copy in y_copies(dz, slot, own, to_after):
                copy.wait_send()
    for k, (source, target) in enumerate(((main_ref, xmain), (tail_ref, xtail))):
        every = pl.ds(0, NZ * group - 1)
        remote(
            source.at[every], target.at[every, :, own], out_send.at[k], out_recv.at[k, 0], higher
        ).wait_send()
    for way in range(2):
        for step in range(4):
            block = pairs.at[0] if step < 3 else pairs.at[0, pl.ds(0, BLOCK), :]
            remote(block, block, kv_send.at[way, step], kv_recv.at[way, step], higher).wait_send()
    for slot in range(9):
        block = pairs.at[0] if slot < 7 else pairs.at[0, pl.ds(0, BLOCK), :]
        remote(block, block, c_send.at[slot], c_recv.at[slot], across).wait_send()
    for slot in range(7):
        remote(
            parts.at[0, 0], parts.at[0, 0], q_send.at[slot], q_recv.at[slot], higher
        ).wait_send()


VMEM = pl.BlockSpec(memory_space=pltpu.VMEM)
HBM = pl.BlockSpec(memory_space=pl.ANY)


def layer_call(
    queries, key_rows, value_rows, head_lambda, sub_gain, out_weight, expert_input, norm_gain,
    route_ids, route_weight, gate, up, down,
):
    dma = pltpu.SemaphoreType.DMA
    slabs, group = NZ * NX * NC, NX * NC
    units = gate.shape[1]
    rows, width = BLOCK // NT, out_weight.shape[1]
    tokens = expert_input.shape[0]
    bf16, f32 = jnp.bfloat16, jnp.float32

    def both(*lead, columns=COLS_T):
        return [pltpu.VMEM((*lead, count, columns), bf16) for count in (FULL, TAIL)]

    return pl.pallas_call(
        layer_kernel,
        out_shape=(
            jax.ShapeDtypeStruct((rows, width), bf16),
            jax.ShapeDtypeStruct((tokens, COLS_T), bf16),
        ),
        in_specs=[pl.BlockSpec(memory_space=pltpu.SMEM)] + [VMEM] * 9 + [HBM] * 3,
        out_specs=(VMEM,) * 2,
        scratch_shapes=[
            *both(slabs),
            pltpu.VMEM((2 * BLOCK, BLOCK), bf16),
            pltpu.VMEM((2, BLOCK, HALF), bf16),
            pltpu.VMEM((tokens, slabs * (FULL + TAIL)), bf16),
            *both(slabs),
            *both(slabs, columns=width),
            pltpu.VMEM((slabs * (FULL + TAIL), width), bf16),
            pltpu.VMEM((slabs * (FULL + TAIL), units), bf16),
            pltpu.VMEM((width, units), bf16),
            pltpu.VMEM((width, units), bf16),
            pltpu.VMEM((units, width), bf16),
            *both(slabs, columns=width),
            pltpu.VMEM((NZ * NC, 2 * BLOCK, BLOCK), bf16),
            pltpu.VMEM((2, NX, BLOCK, HALF), bf16),
            pltpu.VMEM((2, 2, 128, COLS), bf16),
            pltpu.VMEM((2, CHUNK, 256), f32),
            pltpu.VMEM((2, 8, COLS), f32),
            pltpu.VMEM((2, ACC, COLS), f32),
            pltpu.VMEM((NX, 4, ACC, BLOCK), bf16),
            pltpu.VMEM((NX - 1, 4, ACC, BLOCK), bf16),
            pltpu.VMEM((BLOCK, HALF), bf16),
            pltpu.VMEM((BLOCK, HALF), bf16),
            pltpu.VMEM((BLOCK, HALF), bf16),
            pltpu.VMEM((NT, rows, width), bf16),
            pltpu.VMEM((2, rows // 2, width), bf16),
            pltpu.VMEM((2, rows // 2, width), bf16),
            pltpu.VMEM((2, rows, width), bf16),
            *both(NZ, group), *both(NZ, group), *both(2, NZ, group), *both(slabs),
            dma((3,)), dma((4,)), dma((2,)), dma((2, NZ)), dma((3, NZ, 2)), dma((3, NZ, 2)),
            dma((2, 4)), dma((2, 4)), dma((9,)), dma((9,)), dma((7,)), dma((7,)),
            dma((2,)), dma((2, 3)), dma((2, 3)), dma((NZ, 2)), dma((NZ, 2)),
            dma((2, NZ, 2)), dma((2, NZ, 2)), dma((2,)), dma((2,)),
            dma(()), dma(()), dma((2,)), dma((2,)), dma((2, 2)), dma((2, 2)),
        ],
        compiler_params=pltpu.CompilerParams(
            collective_id=0, has_side_effects=True, vmem_limit_bytes=56 * 2**20
        ),
        name="layer",
    )(
        head_lambda, sub_gain[None, :], key_rows, value_rows, queries, expert_input,
        norm_gain[None, :], route_ids.T, route_weight.T, out_weight, gate, up, down,
    )


def shards(
    queries,
    key_rows,
    value_rows,
    head_lambda,
    sub_gain,
    out_weight,
    expert_input,
    norm_gain,
    route_ids,
    route_weight,
    gate_weight,
    up_weight,
    down_weight,
):
    return layer_call(
        queries, key_rows, value_rows, head_lambda, sub_gain, out_weight, expert_input, norm_gain,
        route_ids, route_weight, gate_weight[0], up_weight[0], down_weight[0],
    )


def solution(mesh):
    mesh = Mesh(mesh.devices.reshape(NZ, NX, NC, NT), (*EP, "tp"))
    placed = (
        P(EP, "tp"),
        P(EP, "tp"),
        P(EP, "tp"),
        P("tp"),
        P(),
        P("tp", None),
        P(EP, None),
        P(),
        P(EP, None),
        P(EP, None),
        P(EP, None, "tp"),
        P(EP, None, "tp"),
        P(EP, "tp", None),
    )
    return jax.shard_map(
        shards,
        mesh=mesh,
        in_specs=placed,
        out_specs=(P((*EP, "tp"), None), P(EP, "tp")),
        check_vma=False,
    )
```
